32 devices in a mesh: sp: 8 (over z, x), tp: 4 (over y, core).
Axes of the slice: x: 2, y: 2, z: 4, core: 2. Of those that a mesh axis runs over, the one named last changes fastest.
Arguments:
- residual: bfloat16 [2048, 2048], P('sp', 'tp'), may hold values from -8 to 8
- query_latent: bfloat16 [2048, 512], P('sp'), may hold values from -6 to 6
- shared_latent: bfloat16 [2048, 256], P('sp'), may hold values from -6 to 6
- rotary_key: bfloat16 [2048, 32], P('sp'), may hold values from -300 to 300
- query_gain: float32 [512], replicated, may hold values from 0.1 to 1.9
- latent_gain: float32 [256], replicated, may hold values from 0.1 to 1.9
- query_narrow: bfloat16 [512, 384], P(None, 'tp'), may hold values from -0.5 to 0.5
- key_narrow: bfloat16 [256, 256], P(None, 'tp'), may hold values from -0.375 to 0.375
- value_narrow: bfloat16 [256, 256], P(None, 'tp'), may hold values from -0.375 to 0.375
- query_wide: bfloat16 [512, 640], P(None, 'tp'), may hold values from -0.5 to 0.5
- key_wide: bfloat16 [256, 512], P(None, 'tp'), may hold values from -0.375 to 0.375
- value_wide: bfloat16 [256, 512], P(None, 'tp'), may hold values from -0.375 to 0.375
- output_narrow: bfloat16 [256, 2048], P('tp'), may hold values from -1.75 to 1.75
- output_wide: bfloat16 [512, 2048], P('tp'), may hold values from -1.75 to 1.75
- first_gain: float32 [2048], P('tp'), may hold values from 0.1 to 1.9
- first_bias: float32 [2048], P('tp'), may hold values from -1.5 to 1.5
- gate_weight: bfloat16 [2048, 5632], P('sp', 'tp'), may hold values from -0.125 to 0.125
- up_weight: bfloat16 [2048, 5632], P('sp', 'tp'), may hold values from -0.125 to 0.125
- down_weight: bfloat16 [5632, 2048], P('tp', 'sp'), may hold values from -0.078125 to 0.078125
- second_gain: float32 [2048], P('tp'), may hold values from 0.1 to 1.9
- second_bias: float32 [2048], P('tp'), may hold values from -1.5 to 1.5
Outputs:
- layer_out: bfloat16 [2048, 2048], P('sp', 'tp')
The draws below stay inside these ranges and needn't reach their ends.
All inputs are finite; a program needn't handle non-finite values.
Results may differ from the reference program's by a relative error of at most 0.017.
The reference program's roundings to bfloat16 on the way count: a program that leaves them out, or rounds other values in their place, can miss the bound.
Values may be sent and summed in bfloat16 or wider, within the bound.
A program may use at most 192 MiB of HBM per device.

```python
import math
import jax
import jax.numpy as jnp
from jax import lax

D = 2048
FF = 5632
QL = 512
KVL = 256
ROPE = 32
HEADS_A = 4
HEADS_B = 4
NOPE_A = 64
V_A = 64
NOPE_B = 128
V_B = 128
GRID_W = 64
TOKENS = 2048


def draw_residual(key, part):
    col_scale = jnp.exp(jnp.linspace(math.log(0.5), math.log(1.5), D))
    base = jax.random.normal(key, (TOKENS, D), dtype=jnp.float32) * col_scale
    return jnp.clip(base, -8.0, 8.0).astype(jnp.bfloat16)


def draw_rotary_key(key, part):
    base = jax.random.normal(key, (TOKENS, ROPE), dtype=jnp.float32)
    return jnp.clip(base, -300.0, 300.0).astype(jnp.bfloat16)


def block_levels(stream_key, shape, cuts, least, high):
    level = 1.0
    for dim, blocks in cuts:
        steps = jax.random.uniform(jax.random.fold_in(jax.random.fold_in(stream_key, 6), dim), (blocks,), jnp.float32, least / len(cuts), high / len(cuts))
        level = level * jnp.repeat(jnp.exp(steps), shape[dim] // blocks).reshape((-1,) + (1,) * (len(shape) - 1 - dim))
    return level


def bell_draw(rng, dims, scale, most, shards=(), kind=jnp.bfloat16):
    result = scale * jax.random.normal(rng, dims, jnp.float32)
    if shards:
        result = result * block_levels(rng, dims, shards, -0.22, 0.18)
    return jnp.clip(result, -most, most).astype(kind)


def setup_inputs(seed: int = 0) -> dict:
    seeds = jax.random.split(jax.random.key(seed), 22)
    return {
        "residual": draw_residual(jax.random.fold_in(seeds[21], 71), 0),
        "query_latent": bell_draw(seeds[1], (TOKENS, QL), 1.0, 6.0, ((0, 8),)),
        "shared_latent": bell_draw(seeds[2], (TOKENS, KVL), 1.0, 6.0, ((0, 8),)),
        "rotary_key": draw_rotary_key(jax.random.fold_in(seeds[21], 71), 0),
        "query_gain": jnp.clip(1.0 + 0.18 * jax.random.normal(seeds[4], (QL,), jnp.float32), 0.1, 1.9),
        "latent_gain": jnp.clip(1.0 + 0.18 * jax.random.normal(seeds[5], (KVL,), jnp.float32), 0.1, 1.9),
        "query_narrow": bell_draw(seeds[6], (QL, HEADS_A * (NOPE_A + ROPE)), (QL // 4) ** -0.5, 0.5, ((1, 4),)),
        "key_narrow": bell_draw(seeds[7], (KVL, HEADS_A * NOPE_A), KVL ** -0.5, 0.375, ((1, 4),)),
        "value_narrow": bell_draw(seeds[8], (KVL, HEADS_A * V_A), KVL ** -0.5, 0.375, ((1, 4),)),
        "query_wide": bell_draw(seeds[9], (QL, HEADS_B * (NOPE_B + ROPE)), (QL // 4) ** -0.5, 0.5, ((1, 4),)),
        "key_wide": bell_draw(seeds[10], (KVL, HEADS_B * NOPE_B), KVL ** -0.5, 0.375, ((1, 4),)),
        "value_wide": bell_draw(seeds[11], (KVL, HEADS_B * V_B), KVL ** -0.5, 0.375, ((1, 4),)),
        "output_narrow": bell_draw(seeds[12], (HEADS_A * V_A, D), ((HEADS_A * V_A + HEADS_B * V_B) // 64) ** -0.5, 1.75, ((0, 4),)),
        "output_wide": bell_draw(seeds[13], (HEADS_B * V_B, D), ((HEADS_A * V_A + HEADS_B * V_B) // 64) ** -0.5, 1.75, ((0, 4),)),
        "first_gain": jnp.clip(1.0 + 0.18 * jax.random.normal(seeds[14], (D,), jnp.float32), 0.1, 1.9),
        "first_bias": bell_draw(seeds[15], (D,), 0.3, 1.5, ((0, 4),), jnp.float32),
        "gate_weight": bell_draw(seeds[16], (D, FF), D ** -0.5, 0.125, ((0, 8), (1, 4))),
        "up_weight": bell_draw(seeds[17], (D, FF), D ** -0.5, 0.125, ((0, 8), (1, 4))),
        "down_weight": bell_draw(seeds[18], (FF, D), FF ** -0.5, 0.078125, ((0, 4), (1, 8))),
        "second_gain": jnp.clip(1.0 + 0.18 * jax.random.normal(seeds[19], (D,), jnp.float32), 0.1, 1.9),
        "second_bias": bell_draw(seeds[20], (D,), 0.3, 1.5, ((0, 4),), jnp.float32),
    }


EPS_ROOT = 1e-06
EPS_LAYER = 1e-05
THETA = 10000.0
DEEP_ALPHA = 2.0 ** 0.25

def rotate(half_part, angle):
    lower, upper = jnp.split(half_part, 2, axis=-1)
    cosine = jnp.cos(angle)
    sine = jnp.sin(angle)
    return jnp.concatenate([lower * cosine - upper * sine, upper * cosine + lower * sine], axis=-1)

def turn_axial(values_in, positions):
    quarter = values_in.shape[-1] // 4
    freqs = THETA ** (-(2.0 * jnp.arange(quarter, dtype=jnp.float32)) / (2 * quarter))
    row_angle = (positions // GRID_W).astype(jnp.float32)[:, None, None] * freqs
    col_angle = (positions % GRID_W).astype(jnp.float32)[:, None, None] * freqs
    first_half, second_half = jnp.split(values_in, 2, axis=-1)
    return jnp.concatenate([rotate(first_half, row_angle), rotate(second_half, col_angle)], axis=-1)

def root_scale(latent, gain):
    floated = latent.astype(jnp.float32)
    return floated * lax.rsqrt(lax.optimization_barrier(jnp.mean(floated * floated, axis=-1, keepdims=True)) + EPS_ROOT) * gain.astype(jnp.float32)

def make_query(normed, weight, plain_dim, positions):
    product = jnp.dot(normed, weight, preferred_element_type=jnp.float32)
    head_count = weight.shape[1] // (plain_dim + ROPE)
    product = product.reshape(product.shape[0], head_count, plain_dim + ROPE)
    turned = turn_axial(product[:, :, plain_dim:], positions)
    return jnp.concatenate([product[:, :, :plain_dim], turned], axis=-1).astype(jnp.bfloat16)

def attend(queries, key_rows, value_rows, rotary_rows, plain_dim):
    count, head_count, query_dim = queries.shape
    block_size = math.gcd(count, 512)
    score_scale = query_dim ** (-0.5)
    key_float = key_rows.astype(jnp.float32)
    value_float = value_rows.astype(jnp.float32)
    rotary_float = rotary_rows.astype(jnp.float32)

    def per_block(query_block):
        query_float = query_block.astype(jnp.float32)
        scores = jnp.einsum('qhd,khd->hqk', query_float[:, :, :plain_dim], key_float)
        scores = (scores + jnp.einsum('qhd,kd->hqk', query_float[:, :, plain_dim:], rotary_float)) * score_scale
        largest = lax.optimization_barrier(jnp.max(scores, axis=-1, keepdims=True))
        raised = jnp.exp(scores - largest)
        totals = lax.optimization_barrier(jnp.sum(raised, axis=-1))
        rounded = lax.optimization_barrier(raised.astype(jnp.bfloat16)).astype(jnp.float32)
        output = jnp.einsum('hqk,khd->qhd', rounded, value_float) / totals.T[:, :, None]
        return output.astype(jnp.bfloat16)
    blocks = lax.map(per_block, queries.reshape(count // block_size, block_size, head_count, query_dim))
    return blocks.reshape(count, head_count * value_rows.shape[2])

def layer_norm(summed, gain, bias):
    center = lax.optimization_barrier(jnp.mean(summed, axis=-1, keepdims=True))
    spread = lax.optimization_barrier(jnp.mean((summed - center) * (summed - center), axis=-1, keepdims=True))
    normed = (summed - center) * lax.rsqrt(spread + EPS_LAYER) * gain.astype(jnp.float32) + bias.astype(jnp.float32)
    return normed.astype(jnp.bfloat16)

def reference(residual, query_latent, shared_latent, rotary_key, query_gain, latent_gain, query_narrow, key_narrow, value_narrow, query_wide, key_wide, value_wide, output_narrow, output_wide, first_gain, first_bias, gate_weight, up_weight, down_weight, second_gain, second_bias):
    positions = jnp.arange(residual.shape[0], dtype=jnp.int32)
    query_normed = root_scale(query_latent, query_gain).astype(jnp.bfloat16)
    latent_normed = root_scale(shared_latent, latent_gain).astype(jnp.bfloat16)
    rotary_rows = turn_axial(rotary_key.astype(jnp.float32)[:, None, :], positions)[:, 0, :].astype(jnp.bfloat16)

    def group(query_weight, key_weight, value_weight, plain_dim, value_dim):
        queries = make_query(query_normed, query_weight, plain_dim, positions)
        head_count = queries.shape[1]
        key_rows = jnp.dot(latent_normed, key_weight, preferred_element_type=jnp.float32).astype(jnp.bfloat16)
        value_rows = jnp.dot(latent_normed, value_weight, preferred_element_type=jnp.float32).astype(jnp.bfloat16)
        key_rows = key_rows.reshape(key_rows.shape[0], head_count, plain_dim)
        value_rows = value_rows.reshape(value_rows.shape[0], head_count, value_dim)
        return attend(queries, key_rows, value_rows, rotary_rows, plain_dim)
    attended_narrow = group(query_narrow, key_narrow, value_narrow, NOPE_A, V_A)
    attended_wide = group(query_wide, key_wide, value_wide, NOPE_B, V_B)
    mixed = jnp.dot(attended_narrow, output_narrow, preferred_element_type=jnp.float32)
    mixed = mixed + jnp.dot(attended_wide, output_wide, preferred_element_type=jnp.float32)
    normed_first = layer_norm(DEEP_ALPHA * residual.astype(jnp.float32) + mixed, first_gain, first_bias)
    gate = jnp.dot(normed_first, gate_weight, preferred_element_type=jnp.float32)
    lifted = jnp.dot(normed_first, up_weight, preferred_element_type=jnp.float32)
    hidden = (jax.nn.silu(gate) * lifted).astype(jnp.bfloat16)
    feed = jnp.dot(hidden, down_weight, preferred_element_type=jnp.float32)
    return layer_norm(DEEP_ALPHA * normed_first.astype(jnp.float32) + feed, second_gain, second_bias)
```

```python
import functools

import jax
import jax.numpy as jnp
import numpy as np
from jax import lax
from jax.experimental import pallas as pl
from jax.experimental.pallas import tpu as pltpu
from jax.sharding import PartitionSpec as P

ROPE = 32
NOPE_A = 64
V_A = 64
NOPE_B = 128
V_B = 128
GRID_W = 64

EPS_ROOT = 1e-06
EPS_LAYER = 1e-05
THETA = 10000.0
DEEP_ALPHA = 2.0**0.25

KEY_BLOCK = 2048
ROW_TILE = 16
MESH = pl.DeviceIdType.MESH
BF = jnp.bfloat16
F32 = jnp.float32


def axial_tables(row_total):
    quarter = ROPE // 4
    freqs = np.float32(THETA) ** (-(2.0 * np.arange(quarter, dtype=np.float32)) / (2 * quarter))
    freqs = freqs.astype(np.float32)

    def spread(count, first):
        angle = np.arange(count, dtype=np.float32)[:, None] * freqs
        out = []
        for fn in (np.cos, np.sin):
            table = np.zeros((count, ROPE), np.float32)
            wave = fn(angle).astype(np.float32)
            start = 0 if first else ROPE // 2
            table[:, start : start + quarter] = wave
            table[:, start + quarter : start + 2 * quarter] = wave
            out.append(table)
        return out

    return spread(row_total // GRID_W, True) + spread(GRID_W, False)


def swap_matrix():
    quarter = ROPE // 4
    swap = np.zeros((ROPE, ROPE), np.float32)
    for base in (0, ROPE // 2):
        for i in range(quarter):
            swap[base + quarter + i, base + i] = -1.0
            swap[base + i, base + quarter + i] = 1.0
    return swap


def head_selectors(heads, plain):
    wide = plain + ROPE
    swap = swap_matrix()
    found = []
    for h in range(heads):
        keep = np.zeros((heads * wide, plain), np.float32)
        turn = np.zeros((heads * wide, ROPE), np.float32)
        flip = np.zeros((heads * wide, ROPE), np.float32)
        keep[h * wide : h * wide + plain] = np.eye(plain)
        turn[h * wide + plain : (h + 1) * wide] = np.eye(ROPE)
        flip[h * wide + plain : (h + 1) * wide] = swap
        found.append((keep, turn, flip))
    return [np.stack(group) for group in zip(*found)]


def split_groups(device_count, hidden_local, width, row_count):
    best = None
    for groups in range(1, device_count + 1):
        if device_count % groups or hidden_local % groups:
            continue
        moved = 3 * width * hidden_local // groups + 2 * row_count * groups * width
        if best is None or moved < best[0]:
            best = (moved, groups)
    return best[1]


def other(index, bit):
    return index + bit * (1 - 2 * ((index // bit) % 2))


def send(source, target, send_sem, recv_sem, sp, tp):
    return pltpu.make_async_remote_copy(
        src_ref=source,
        dst_ref=target,
        send_sem=send_sem,
        recv_sem=recv_sem,
        device_id={"sp": sp, "tp": tp},
        device_id_type=MESH,
    )


def dot(a, b):
    return jnp.dot(a, b, preferred_element_type=F32)


def across_dot(rows, columns):
    return lax.dot_general(
        rows, columns, (((1,), (1,)), ((), ())), preferred_element_type=F32
    )


def root_norm(values, gain):
    return values * lax.rsqrt(jnp.mean(values * values, axis=-1, keepdims=True) + EPS_ROOT) * gain


def layer_norm(values, gain, bias):
    center = jnp.mean(values, axis=-1, keepdims=True)
    moved = values - center
    spread = jnp.mean(moved * moved, axis=-1, keepdims=True)
    return moved * lax.rsqrt(spread + EPS_LAYER) * gain + bias


def layer_kernel(groups, turns, parts, *refs):
    (
        residual, query_latent, shared_latent, rotary_key, query_gain, latent_gain,
        query_narrow, key_narrow, value_narrow, query_wide, key_wide, value_wide,
        output_narrow, output_wide, first_gain, first_bias,
        gate_weight, up_weight, down_weight, second_gain, second_bias,
        row_cos, row_sin, col_cos, col_sin, swap, eye,
        keep_n, turn_n, flip_n, keep_w, turn_w, flip_w,
    ) = refs[:33]
    out_ref = refs[33]
    (
        raw, staged, weights, latents, cosine, sine, parts_f, raised, vals_n, vals_w,
        tops, totals, sums_n, sums_w, out_n, out_w, res_all, own_gains, gains,
        att_n, att_w, x_all, hidden, s1, r1, s2, r2, s3, r3, final,
    ) = refs[34:64]
    (
        load_sem, lzs, lzr, lxs, lxr, lcs, lcr, wzs, wzr, wxs, wxr, wls,
        tps, tpr, gns, gnr, ags, agr, ars, arr, p1s, p1r, p2s, p2r, p3s, p3r, fs, fr, fl,
    ) = refs[64:]
    sp, tp = lax.axis_index("sp"), lax.axis_index("tp")
    count = groups * turns
    group, turn = sp // turns, sp % turns
    low, high = tp % 2, tp // 2
    near, far = other(tp, 1), other(tp, 2)
    diag = other(far, 1)
    rows = query_latent.shape[0]
    width = x_all.shape[2]
    hidden_count, depth = weights.shape[2], weights.shape[3]
    quarter = rows // parts
    tail = []

    def group_at(k):
        return ((group + k) % groups) * turns + turn

    def turn_at(j):
        return group * turns + (turn + j) % turns

    def source_at(k, j):
        return ((group - k + groups) % groups) * turns + (turn - j + turns) % turns

    loads = []
    for i, (source, target) in enumerate(
        (
            (gate_weight, raw.at[0]),
            (up_weight, raw.at[1]),
            (down_weight, staged.at[2]),
            (output_narrow, out_n.at[tp]),
            (output_wide, out_w.at[tp]),
            (residual, res_all.at[tp]),
        )
    ):
        load = pltpu.make_async_copy(source, target, load_sem.at[i])
        load.start()
        loads.append(load)

    barrier = pltpu.get_barrier_semaphore()
    peers = [(group_at(k), tp) for k in range(1, groups)]
    peers += [(turn_at(j), tp) for j in range(1, turns)]
    peers += [(sp, near), (sp, far), (sp, diag)]
    for a, b in peers:
        pl.semaphore_signal(barrier, inc=1, device_id={"sp": a, "tp": b}, device_id_type=MESH)

    grid_rows = rows // GRID_W
    for i in range(grid_rows):
        at = pl.ds(i * GRID_W, GRID_W)
        line = pl.ds(sp * grid_rows + i, 1)
        cosine[at, :] = col_cos[...] + row_cos[line, :]
        sine[at, :] = col_sin[...] + row_sin[line, :]
    latents[sp, 0:rows, :] = root_norm(shared_latent[...].astype(F32), latent_gain[...]).astype(BF)
    rotary = rotary_key[...]
    turned = rotary.astype(F32) * cosine[...] + dot(rotary, swap[...]) * sine[...]
    latents[sp, rows : rows + ROPE, :] = across_dot(eye[...], turned.astype(BF)).astype(BF)
    for i, ref in enumerate((first_gain, first_bias, second_gain, second_bias)):
        own_gains[i : i + 1, :] = ref[...]
        gains[tp, i : i + 1, :] = ref[...]
    pl.semaphore_wait(barrier, len(peers))

    half = (rows + ROPE) // 2
    part = pl.ds(pl.multiple_of(low * half, half), half)
    lat_copies = []
    for k in range(1, groups):
        block = latents.at[sp, part]
        copy = send(block, block, lzs.at[k], lzr.at[k], group_at(k), tp)
        copy.start()
        lat_copies.append(copy)
    for j in range(1, turns):
        block = latents.at[sp, part]
        copy = send(block, block, lxs.at[0, j], lxr.at[0, j], turn_at(j), tp)
        copy.start()
        tail.append(copy.wait_send)

    def share(source, target, i):
        a = send(source, target.at[tp], tps.at[i, 0], tpr.at[i, 0], sp, far)
        b = send(source, target.at[tp], tps.at[i, 1], tpr.at[i, 1], sp, near)
        a.start()
        b.start()
        tail.append(a.wait_send)
        tail.append(b.wait_send)

        def onward():
            a.wait_recv()
            c = send(target.at[far], target.at[far], tps.at[i, 2], tpr.at[i, 2], sp, near)
            c.start()
            tail.append(c.wait_send)

            def done():
                b.wait_recv()
                c.wait_recv()

            return done

        return onward

    onward = [share(output_wide, out_w, 0), share(output_narrow, out_n, 1), share(residual, res_all, 2)]
    gain_copies = []
    for i, peer in enumerate((near, far, diag)):
        copy = send(own_gains, gains.at[tp], gns.at[i], gnr.at[i], sp, peer)
        copy.start()
        gain_copies.append(copy)
        tail.append(copy.wait_send)

    loads[0].wait()
    staged[0] = raw[0].T
    loads[1].wait()
    staged[1] = raw[1].T
    loads[2].wait()

    def piece(m, k):
        first = pl.multiple_of(((group + k) % groups) * hidden_count, 16)
        return staged.at[m, pl.ds(first, hidden_count)]

    weight_z = {}

    def send_weights(m):
        for k in range(1, groups):
            copy = send(piece(m, k), weights.at[m, sp], wzs.at[m, k], wzr.at[m, k], group_at(k), tp)
            copy.start()
            tail.append(copy.wait_send)
            weight_z[m, k] = copy
        local = pltpu.make_async_copy(piece(m, 0), weights.at[m, sp], wls.at[m])
        local.start()
        weight_z[m, 0] = local

    weight_x = {}

    def pass_weights(m, k):
        if k:
            weight_z[m, k].wait_recv()
        source = source_at(k, 0)
        block = weights.at[m, source] if k else piece(m, 0)
        for j in range(1, turns):
            copy = send(block, weights.at[m, source], wxs.at[m, k, j], wxr.at[m, k, j], turn_at(j), tp)
            copy.start()
            tail.append(copy.wait_send)
            weight_x[m, k, j] = copy

    def weights_here(m):
        weight_z[m, 0].wait()
        for k in range(groups):
            for j in range(1, turns):
                weight_x[m, k, j].wait_recv()

    send_weights(0)
    send_weights(1)

    shares = []

    def to_mate(k, j):
        block = latents.at[source_at(k, j), part]
        copy = send(block, block, lcs.at[k, j], lcr.at[k, j], sp, near)
        copy.start()
        tail.append(copy.wait_send)
        shares.append(copy)

    def latent_x(k, j):
        block = latents.at[sp, part]
        return send(block, block, lxs.at[k, j], lxr.at[k, j], turn_at(j), tp)

    for k in range(1, groups):
        lat_copies[k - 1].wait_recv()
        tail.append(lat_copies[k - 1].wait_send)
        block = latents.at[source_at(k, 0), part]
        for j in range(1, turns):
            copy = send(block, block, lxs.at[k, j], lxr.at[k, j], turn_at(j), tp)
            copy.start()
            tail.append(copy.wait_send)
        to_mate(k, 0)
    for m in range(2):
        pass_weights(m, 0)

    normed = root_norm(query_latent[...].astype(F32), query_gain[...]).astype(BF)
    scales = []
    heads = []
    for weight, keep, turns_m, flips, key_w, value_w, vals, sums, att, plain, value_dim in (
        (query_narrow, keep_n, turn_n, flip_n, key_narrow, value_narrow, vals_n, sums_n, att_n, NOPE_A, V_A),
        (query_wide, keep_w, turn_w, flip_w, key_wide, value_wide, vals_w, sums_w, att_w, NOPE_B, V_B),
    ):
        for h in range(keep.shape[0]):
            whole = weight[...]
            plain_q = dot(normed, dot(whole, keep[h]).astype(BF)).astype(BF)
            turn_q = dot(normed, dot(whole, turns_m[h]).astype(BF))
            flip_q = dot(normed, dot(whole, flips[h]).astype(BF))
            turn_q = (turn_q * cosine[...] + flip_q * sine[...]).astype(BF)
            heads.append((plain_q, turn_q, key_w, value_w, vals, sums, att, h, plain, value_dim))

    for k in range(groups):
        for j in range(1, turns):
            latent_x(k, j).wait_recv()
            to_mate(k, j)
    for copy in shares:
        copy.wait_recv()

    per = min(KEY_BLOCK // rows, count)
    blocks = count // per
    for n in range(len(heads)):
        tops[n] = jnp.full(tops.shape[1:], -jnp.inf, F32)
        totals[n] = jnp.zeros(totals.shape[1:], F32)
    sums_n[...] = jnp.zeros(sums_n.shape, F32)
    sums_w[...] = jnp.zeros(sums_w.shape, F32)

    def attend(b, carry):
        for n, (plain_q, turn_q, key_w, value_w, vals, sums, att, h, plain, value_dim) in enumerate(heads):
            for s in range(per):
                shard = b * per + s
                rows_here = latents[shard, 0:rows, :]
                keys = dot(rows_here, key_w[:, h * plain : (h + 1) * plain]).astype(BF)
                scores = across_dot(plain_q, keys) + dot(turn_q, latents[shard, rows : rows + ROPE, :])
                parts_f[n, :, s * rows : (s + 1) * rows] = scores
                vals[s * rows : (s + 1) * rows, :] = dot(
                    rows_here, value_w[:, h * value_dim : (h + 1) * value_dim]
                ).astype(BF)
            scale = (plain + ROPE) ** (-0.5)

            def tile(i, inner):
                at = pl.ds(pl.multiple_of(i * ROW_TILE, ROW_TILE), ROW_TILE)
                scores = parts_f[n, at, 0 : per * rows] * scale
                before = tops[n, at, :]
                largest = jnp.maximum(before[:, 0:1], jnp.max(scores, axis=-1, keepdims=True))
                lifted = jnp.exp(scores - largest)
                factor = jnp.exp(before - largest)
                tops[n, at, :] = jnp.broadcast_to(largest, before.shape)
                totals[n, at, :] = totals[n, at, :] * factor + jnp.sum(lifted, axis=-1, keepdims=True)
                raised[at, 0 : per * rows] = lifted.astype(BF)
                here = sums[h, at, :]
                sums[h, at, :] = here * factor[:, 0:1]
                return inner

            lax.fori_loop(0, rows // ROW_TILE, tile, 0)
            sums[h] = sums[h] + dot(raised[:, 0 : per * rows], vals[...])
        return carry

    if blocks == 1:
        attend(0, 0)
    else:
        lax.fori_loop(0, blocks, attend, 0)
    for n, (_, _, _, _, _, sums, att, h, _, value_dim) in enumerate(heads):
        att[tp, :, h * value_dim : (h + 1) * value_dim] = (sums[h] / totals[n][:, 0:1]).astype(BF)

    rest = [att_onward for att_onward in (share(att_w.at[tp], att_w, 3), share(att_n.at[tp], att_n, 4))]
    done = [step() for step in onward]
    for k in range(1, groups):
        pass_weights(0, k)
    done += [step() for step in rest]
    for step in done:
        step()
    for i in range(3, 6):
        loads[i].wait()
    for copy in gain_copies:
        copy.wait_recv()

    block_w = width // parts
    for c in range(parts):
        at = slice(c * block_w, (c + 1) * block_w)
        mixed = DEEP_ALPHA * res_all[c].astype(F32)
        for t in range(parts):
            mixed = mixed + dot(att_n[t], out_n[t, :, at])
            mixed = mixed + dot(att_w[t], out_w[t, :, at])
        parts_f[0, :, at] = mixed
    gain1 = jnp.concatenate([gains[t, 0:1, :] for t in range(parts)], axis=1)
    bias1 = jnp.concatenate([gains[t, 1:2, :] for t in range(parts)], axis=1)

    def first_norm(i, inner):
        at = pl.ds(pl.multiple_of(i * ROW_TILE, ROW_TILE), ROW_TILE)
        x_all[0, at, :] = layer_norm(parts_f[0, at, :], gain1, bias1).astype(BF)
        return inner

    lax.fori_loop(0, rows // ROW_TILE, first_norm, 0)

    def strip(t):
        return pl.ds(pl.multiple_of(t * quarter, quarter), quarter)

    ahead = [None]
    send_weights(2)
    pass_weights(2, 0)
    for k in range(1, groups):
        copy = send(
            x_all.at[0, strip(tp)], x_all.at[k, strip(tp)], ags.at[k], agr.at[k], group_at(k), tp
        )
        copy.start()
        tail.append(copy.wait_send)
        ahead.append(copy)
    for k in range(1, groups):
        pass_weights(1, k)
    for k in range(1, groups):
        pass_weights(2, k)

    relayed = {}

    def relay(k):
        ahead[k].wait_recv()
        block = x_all.at[k, strip(tp)]
        for i, peer in ((0, far), (1, near)):
            copy = send(block, block, ars.at[k, i], arr.at[k, i], sp, peer)
            copy.start()
            tail.append(copy.wait_send)
            relayed[k, i] = copy

    def relay_far(k):
        relayed[k, 0].wait_recv()
        block = x_all.at[k, strip(far)]
        copy = send(block, block, ars.at[k, 2], arr.at[k, 2], sp, near)
        copy.start()
        tail.append(copy.wait_send)
        relayed[k, 2] = copy

    firsts, seconds, thirds = [], [], [None]

    def compute(k):
        if k:
            relayed[k, 1].wait_recv()
            relayed[k, 2].wait_recv()
        if k == 0:
            weights_here(0)
            weights_here(1)
        gate = jnp.zeros((rows, hidden_count), F32)
        lifted = gate
        for i in range(count):
            columns = x_all[k, :, i * depth : (i + 1) * depth]
            gate += across_dot(columns, weights[0, i])
            lifted += across_dot(columns, weights[1, i])
        hidden[k] = (jax.nn.silu(gate) * lifted).astype(BF)

    def down(k):
        if k == 0:
            weights_here(2)
        for i in range(count):
            parts_f[k, :, i * depth : (i + 1) * depth] = dot(hidden[k], weights[2, i])
        for h in range(2):
            s1[k, h] = parts_f[k, strip(2 * h + 1 - low), :].astype(BF)
        firsts.append(send(s1.at[k], r1.at[k], p1s.at[k], p1r.at[k], sp, near))
        firsts[k].start()
        tail.append(firsts[k].wait_send)

    def second(k):
        firsts[k].wait_recv()
        kept = parts_f[k, strip(2 * (1 - high) + low), :]
        s2[k] = (kept + r1[k, 1 - high].astype(F32)).astype(BF)
        seconds.append(send(s2.at[k], r2.at[k], p2s.at[k], p2r.at[k], sp, far))
        seconds[k].start()
        tail.append(seconds[k].wait_send)

    def third(k):
        seconds[k].wait_recv()
        total = parts_f[k, strip(tp), :] + r1[k, high].astype(F32) + r2[k].astype(F32)
        if k == 0:
            parts_f[0, strip(tp), :] = total
        else:
            s3[k] = total.astype(BF)
            owner = source_at(k, 0)
            thirds.append(send(s3.at[k], r3.at[k], p3s.at[k], p3r.at[k], owner, tp))
            thirds[k].start()
            tail.append(thirds[k].wait_send)

    if groups > 1:
        relay(1)
    compute(0)
    if groups > 1:
        relay_far(1)
    for k in range(groups):
        if k + 2 < groups:
            relay(k + 2)
        down(k)
        if k + 1 < groups:
            compute(k + 1)
        if k + 2 < groups:
            relay_far(k + 2)
        second(k)
        if k >= 1:
            third(k - 1)
    third(groups - 1)

    for k in range(1, groups):
        thirds[k].wait_recv()
    gain2 = jnp.concatenate([gains[t, 2:3, :] for t in range(parts)], axis=1)
    bias2 = jnp.concatenate([gains[t, 3:4, :] for t in range(parts)], axis=1)
    for i in range(quarter // ROW_TILE):
        base = pl.multiple_of(tp * quarter + i * ROW_TILE, ROW_TILE)
        at = slice(i * ROW_TILE, (i + 1) * ROW_TILE)
        total = parts_f[0, pl.ds(base, ROW_TILE), :]
        for k in range(1, groups):
            total = total + r3[k, at, :].astype(F32)
        total = total + DEEP_ALPHA * x_all[0, pl.ds(base, ROW_TILE), :].astype(F32)
        result = layer_norm(total, gain2, bias2).astype(BF)
        for c in range(parts):
            final[c, at, :] = result[:, c * block_w : (c + 1) * block_w]
    finals = []
    for i, peer in enumerate((far, diag, near)):
        copy = send(final.at[peer], out_ref.at[strip(tp)], fs.at[i], fr.at[i], sp, peer)
        copy.start()
        finals.append(copy)
    local = pltpu.make_async_copy(final.at[tp], out_ref.at[strip(tp)], fl)
    local.start()
    for copy in finals:
        copy.wait_recv()
        copy.wait_send()
    local.wait()
    for wait in tail:
        wait()


def whole_layer(args, constants, groups, turns, parts):
    (
        residual, query_latent, shared_latent, rotary_key, query_gain, latent_gain,
        query_narrow, key_narrow, value_narrow, query_wide, key_wide, value_wide,
        output_narrow, output_wide, first_gain, first_bias,
        gate_weight, up_weight, down_weight, second_gain, second_bias,
    ) = args
    count = groups * turns
    rows, own_width = residual.shape
    width = own_width * parts
    depth, hidden_local = gate_weight.shape
    hidden_count = hidden_local // groups
    heads_n, heads_w = key_narrow.shape[1] // NOPE_A, key_wide.shape[1] // NOPE_B
    heads = heads_n + heads_w
    quarter = rows // parts
    keys = min(KEY_BLOCK, count * rows)
    latent_width = shared_latent.shape[1]
    dma = pltpu.SemaphoreType.DMA
    vm, far_ref = pl.BlockSpec(memory_space=pltpu.VMEM), pl.BlockSpec(memory_space=pl.ANY)
    names = [vm] * 21
    for i in (0, 12, 13, 16, 17, 18):
        names[i] = far_ref
    strip = (quarter, width)
    return pl.pallas_call(
        functools.partial(layer_kernel, groups, turns, parts),
        out_shape=jax.ShapeDtypeStruct(residual.shape, BF),
        in_specs=names + [vm] * len(constants),
        out_specs=vm,
        scratch_shapes=[
            pltpu.VMEM((2, depth, hidden_local), BF),
            pltpu.VMEM((3, hidden_local, depth), BF),
            pltpu.VMEM((3, count, hidden_count, depth), BF),
            pltpu.VMEM((count, rows + ROPE, latent_width), BF),
            pltpu.VMEM((rows, ROPE), F32),
            pltpu.VMEM((rows, ROPE), F32),
            pltpu.VMEM((max(groups, heads), rows, max(width, keys)), F32),
            pltpu.VMEM((rows, keys), BF),
            pltpu.VMEM((keys, V_A), BF),
            pltpu.VMEM((keys, V_B), BF),
            pltpu.VMEM((heads, rows, 128), F32),
            pltpu.VMEM((heads, rows, 128), F32),
            pltpu.VMEM((heads_n, rows, V_A), F32),
            pltpu.VMEM((heads_w, rows, V_B), F32),
            pltpu.VMEM((parts,) + output_narrow.shape, BF),
            pltpu.VMEM((parts,) + output_wide.shape, BF),
            pltpu.VMEM((parts,) + residual.shape, BF),
            pltpu.VMEM((8, own_width), F32),
            pltpu.VMEM((parts, 8, own_width), F32),
            pltpu.VMEM((parts, rows, heads_n * V_A), BF),
            pltpu.VMEM((parts, rows, heads_w * V_B), BF),
            pltpu.VMEM((groups, rows, width), BF),
            pltpu.VMEM((groups, rows, hidden_count), BF),
            pltpu.VMEM((groups, 2) + strip, BF),
            pltpu.VMEM((groups, 2) + strip, BF),
            pltpu.VMEM((groups,) + strip, BF),
            pltpu.VMEM((groups,) + strip, BF),
            pltpu.VMEM((groups,) + strip, BF),
            pltpu.VMEM((groups,) + strip, BF),
            pltpu.VMEM((parts, quarter, own_width), BF),
            dma((6,)),
            dma((groups,)),
            dma((groups,)),
            dma((groups, turns)),
            dma((groups, turns)),
            dma((groups, turns)),
            dma((groups, turns)),
            dma((3, groups)),
            dma((3, groups)),
            dma((3, groups, turns)),
            dma((3, groups, turns)),
            dma((3,)),
            dma((5, 3)),
            dma((5, 3)),
            dma((3,)),
            dma((3,)),
            dma((groups,)),
            dma((groups,)),
            dma((groups, 3)),
            dma((groups, 3)),
            dma((groups,)),
            dma((groups,)),
            dma((groups,)),
            dma((groups,)),
            dma((groups,)),
            dma((groups,)),
            dma((3,)),
            dma((3,)),
            dma(()),
        ],
        compiler_params=pltpu.CompilerParams(
            collective_id=0, has_side_effects=True, vmem_limit_bytes=62 * 2**20
        ),
        name="layer",
    )(*args, *constants)


def body(*args):
    args = [a.reshape(1, -1) if a.ndim == 1 else a for a in args]
    rows, own_width = args[0].shape
    device_count, parts = lax.axis_size("sp"), lax.axis_size("tp")
    hidden_local = args[16].shape[1]
    groups = split_groups(device_count, hidden_local, own_width * parts, rows)
    turns = device_count // groups
    constants = [jnp.asarray(t) for t in axial_tables(rows * device_count)]
    constants += [jnp.asarray(t, BF) for t in (swap_matrix(), np.eye(ROPE))]
    for weight, plain in ((args[6], NOPE_A), (args[9], NOPE_B)):
        heads = weight.shape[1] // (plain + ROPE)
        constants += [jnp.asarray(t, BF) for t in head_selectors(heads, plain)]
    return whole_layer(args, constants, groups, turns, parts)


def solution(mesh):
    return jax.shard_map(
        body,
        mesh=mesh,
        in_specs=(
            P("sp", "tp"),
            P("sp", None),
            P("sp", None),
            P("sp", None),
            P(),
            P(),
            P(None, "tp"),
            P(None, "tp"),
            P(None, "tp"),
            P(None, "tp"),
            P(None, "tp"),
            P(None, "tp"),
            P("tp", None),
            P("tp", None),
            P("tp"),
            P("tp"),
            P("sp", "tp"),
            P("sp", "tp"),
            P("tp", "sp"),
            P("tp"),
            P("tp"),
        ),
        out_specs=P("sp", "tp"),
        check_vma=False,
    )
```

```python
import functools

import jax
import jax.numpy as jnp
import numpy as np
from jax import lax
from jax.experimental import pallas as pl
from jax.experimental.pallas import tpu as pltpu
from jax.sharding import PartitionSpec as P

ROPE = 32
NOPE_A = 64
V_A = 64
NOPE_B = 128
V_B = 128
GRID_W = 64

EPS_ROOT = 1e-06
EPS_LAYER = 1e-05
THETA = 10000.0
DEEP_ALPHA = 2.0**0.25

KEY_BLOCK = 2048
ROW_TILE = 16
MESH = pl.DeviceIdType.MESH
BF = jnp.bfloat16
F32 = jnp.float32


def axial_tables(row_total):
    quarter = ROPE // 4
    freqs = np.float32(THETA) ** (-(2.0 * np.arange(quarter, dtype=np.float32)) / (2 * quarter))
    freqs = freqs.astype(np.float32)

    def spread(count, first):
        angle = np.arange(count, dtype=np.float32)[:, None] * freqs
        out = []
        for fn in (np.cos, np.sin):
            table = np.zeros((count, ROPE), np.float32)
            wave = fn(angle).astype(np.float32)
            start = 0 if first else ROPE // 2
            table[:, start : start + quarter] = wave
            table[:, start + quarter : start + 2 * quarter] = wave
            out.append(table)
        return out

    return spread(row_total // GRID_W, True) + spread(GRID_W, False)


def swap_matrix():
    quarter = ROPE // 4
    swap = np.zeros((ROPE, ROPE), np.float32)
    for base in (0, ROPE // 2):
        for i in range(quarter):
            swap[base + i, base + quarter + i] = -1.0
            swap[base + quarter + i, base + i] = 1.0
    return swap


def split_groups(device_count, hidden_local, width, row_count):
    best = None
    for groups in range(1, device_count + 1):
        if device_count % groups or hidden_local % groups:
            continue
        moved = 3 * width * hidden_local // groups + 2 * row_count * groups * width
        if best is None or moved < best[0]:
            best = (moved, groups)
    return best[1]


def other(index, bit):
    return index + bit * (1 - 2 * ((index // bit) % 2))


def send(source, target, send_sem, recv_sem, sp, tp):
    return pltpu.make_async_remote_copy(
        src_ref=source,
        dst_ref=target,
        send_sem=send_sem,
        recv_sem=recv_sem,
        device_id={"sp": sp, "tp": tp},
        device_id_type=MESH,
    )


def dot(a, b):
    return jnp.dot(a, b, preferred_element_type=F32)


def across_dot(rows, columns):
    return lax.dot_general(
        rows, columns, (((1,), (1,)), ((), ())), preferred_element_type=F32
    )


def root_norm(values, gain):
    return values * lax.rsqrt(jnp.mean(values * values, axis=-1, keepdims=True) + EPS_ROOT) * gain


def layer_norm(values, gain, bias):
    center = jnp.mean(values, axis=-1, keepdims=True)
    moved = values - center
    spread = jnp.mean(moved * moved, axis=-1, keepdims=True)
    return moved * lax.rsqrt(spread + EPS_LAYER) * gain + bias


def chain_orders(groups):
    found = []
    for g in range(groups):
        found.append(sorted(range(groups), key=lambda s: (abs(s - g), s)))
    return found


def pick(index, options):
    value = options[-1]
    for i, option in enumerate(options[:-1]):
        value = jnp.where(index == i, option, value)
    return value


def layer_kernel(groups, turns, parts, *refs):
    (
        residual, query_latent, shared_latent, rotary_key, query_gain, latent_gain,
        query_narrow, key_narrow, value_narrow, query_wide, key_wide, value_wide,
        output_narrow, output_wide, first_gain, first_bias,
        gate_weight, up_weight, down_weight, second_gain, second_bias,
        row_cos, row_sin, col_cos, col_sin, swap,
    ) = refs[:26]
    out_ref = refs[26]
    (
        raw, staged, weights, latents, cosine, sine, board, parts_f, raised, key_all, value_all, vals,
        peaks, tops, totals, sums, out_n, out_w, res_all, own_gains, gains,
        att_n, att_w, x_all, hidden, s1, r1, s2, r2, s3, r3, final,
    ) = refs[27:59]
    (
        load_sem, lzs, lzr, lxs, lxr, lcs, lcr, wzs, wzr, wxs, wxr, wls,
        tps, tpr, gns, gnr, ags, agr, ars, arr, p1s, p1r, p2s, p2r, p3s, p3r, fs, fr, fl,
    ) = refs[59:]
    sp, tp = lax.axis_index("sp"), lax.axis_index("tp")
    count = groups * turns
    group, turn = sp // turns, sp % turns
    low, high = tp % 2, tp // 2
    near, far = other(tp, 1), other(tp, 2)
    diag = other(far, 1)
    rows = query_latent.shape[0]
    width = residual.shape[1] * parts
    hidden_count, depth = weights.shape[2], weights.shape[3]
    quarter = rows // parts
    orders = chain_orders(groups)
    sources = [group] + [pick(group, [orders[g][k] for g in range(groups)]) for k in range(1, groups)]
    heads_w, heads_n = key_wide.shape[1] // NOPE_B, key_narrow.shape[0] // NOPE_A
    tail = []

    def group_at(k):
        return ((group + k) % groups) * turns + turn

    def turn_at(j):
        return group * turns + (turn + j) % turns

    def source_at(k, j):
        return ((group - k + groups) % groups) * turns + (turn - j + turns) % turns

    wide_v, narrow_v = heads_w * V_B, heads_n * V_A
    own_w = pl.ds(pl.multiple_of(tp * wide_v, 16), wide_v)
    own_n = pl.ds(pl.multiple_of(tp * narrow_v, 16), narrow_v)
    loads = []
    for i, (source, target) in enumerate(
        (
            (gate_weight, raw.at[0]),
            (up_weight, raw.at[1]),
            (down_weight, staged.at[2]),
            (output_narrow, out_n.at[own_n]),
            (output_wide, out_w.at[own_w]),
            (residual, res_all.at[tp]),
        )
    ):
        load = pltpu.make_async_copy(source, target, load_sem.at[i])
        load.start()
        loads.append(load)

    barrier = pltpu.get_barrier_semaphore()
    peers = [(group_at(k), tp) for k in range(1, groups)]
    peers += [(turn_at(j), tp) for j in range(1, turns)]
    peers += [(sp, near), (sp, far), (sp, diag)]
    for a, b in peers:
        pl.semaphore_signal(barrier, inc=1, device_id={"sp": a, "tp": b}, device_id_type=MESH)

    grid_rows = rows // GRID_W
    for i in range(grid_rows):
        at = pl.ds(i * GRID_W, GRID_W)
        line = pl.ds(sp * grid_rows + i, 1)
        cosine[at, :] = col_cos[...] + row_cos[line, :]
        sine[at, :] = col_sin[...] + row_sin[line, :]
    latents[sp, 0:rows, :] = root_norm(shared_latent[...].astype(F32), latent_gain[...]).astype(BF)
    rotary = rotary_key[...]
    turned = rotary.astype(F32) * cosine[...].T + dot(swap[...], rotary) * sine[...].T
    latents[sp, rows : rows + ROPE, :] = turned.astype(BF)
    own_gains[...] = jnp.zeros(own_gains.shape, F32)
    for i, ref in enumerate((first_gain, first_bias, second_gain, second_bias)):
        own_gains[i : i + 1, :] = ref[...]
        gains[tp, i : i + 1, :] = ref[...]
    pl.semaphore_wait(barrier, len(peers))

    half = (rows + ROPE) // 2
    part = pl.ds(pl.multiple_of(low * half, half), half)
    lat_copies = []
    for k in range(1, groups):
        block = latents.at[sp, part]
        copy = send(block, block, lzs.at[k], lzr.at[k], group_at(k), tp)
        copy.start()
        lat_copies.append(copy)
    for j in range(1, turns):
        block = latents.at[sp, part]
        copy = send(block, block, lxs.at[0, j], lxr.at[0, j], turn_at(j), tp)
        copy.start()
        tail.append(copy.wait_send)

    def share(source, view, i):
        a = send(source, view(tp), tps.at[i, 0], tpr.at[i, 0], sp, far)
        b = send(source, view(tp), tps.at[i, 1], tpr.at[i, 1], sp, near)
        a.start()
        b.start()
        tail.append(a.wait_send)
        tail.append(b.wait_send)

        def onward():
            a.wait_recv()
            c = send(view(far), view(far), tps.at[i, 2], tpr.at[i, 2], sp, near)
            c.start()
            tail.append(c.wait_send)

            def done():
                b.wait_recv()
                c.wait_recv()

            return done

        return onward

    onward = [
        share(output_wide, lambda t: out_w.at[pl.ds(pl.multiple_of(t * wide_v, 16), wide_v)], 0),
        share(output_narrow, lambda t: out_n.at[pl.ds(pl.multiple_of(t * narrow_v, 16), narrow_v)], 1),
        share(residual, lambda t: res_all.at[t], 2),
    ]
    gain_copies = []
    for i, peer in enumerate((near, far, diag)):
        copy = send(own_gains, gains.at[tp], gns.at[i], gnr.at[i], sp, peer)
        copy.start()
        gain_copies.append(copy)
        tail.append(copy.wait_send)

    loads[0].wait()
    staged[0] = raw[0].T
    loads[1].wait()
    staged[1] = raw[1].T
    loads[2].wait()

    def piece(m, k):
        first = pl.multiple_of(((group + k) % groups) * hidden_count, 16)
        return staged.at[m, pl.ds(first, hidden_count)]

    weight_z = {}

    def send_weights(m):
        for k in range(1, groups):
            copy = send(piece(m, k), weights.at[m, sp], wzs.at[m, k], wzr.at[m, k], group_at(k), tp)
            copy.start()
            tail.append(copy.wait_send)
            weight_z[m, k] = copy
        local = pltpu.make_async_copy(piece(m, 0), weights.at[m, sp], wls.at[m])
        local.start()
        weight_z[m, 0] = local

    weight_x = {}

    def pass_weights(m, k):
        if k:
            weight_z[m, k].wait_recv()
        source = source_at(k, 0)
        block = weights.at[m, source] if k else piece(m, 0)
        for j in range(1, turns):
            copy = send(block, weights.at[m, source], wxs.at[m, k, j], wxr.at[m, k, j], turn_at(j), tp)
            copy.start()
            tail.append(copy.wait_send)
            weight_x[m, k, j] = copy

    def weights_here(m, k):
        if k == 0:
            weight_z[m, 0].wait()
        for j in range(1, turns):
            weight_x[m, k, j].wait_recv()

    send_weights(0)
    send_weights(1)

    normed = root_norm(query_latent[...].astype(F32), query_gain[...]).astype(BF)
    heads = []
    for weight, plain, value_dim, head_count, first_key, first_value in (
        (query_wide, NOPE_B, V_B, heads_w, 0, 0),
        (query_narrow, NOPE_A, V_A, heads_n, heads_w * NOPE_B, wide_v),
    ):
        for h in range(head_count):
            first = h * (plain + ROPE)
            turn_w = weight[first + plain : first + plain + ROPE, :]
            plain_q = across_dot(normed, weight[first : first + plain, :]).astype(BF)
            turn_q = across_dot(normed, turn_w)
            flip_q = across_dot(normed, dot(swap[...], turn_w).astype(BF))
            turn_q = (turn_q * cosine[...] + flip_q * sine[...]).astype(BF)
            query = jnp.concatenate([plain_q, turn_q], axis=1)
            heads.append((query, plain, value_dim, first_key + h * plain, first_value + h * value_dim))
    key_all[0 : heads_w * NOPE_B, :] = key_wide[...].T
    key_all[heads_w * NOPE_B :, :] = key_narrow[...]
    value_all[:, 0:wide_v] = value_wide[...]
    value_all[:, wide_v:] = value_narrow[...].T

    shares = {}

    def to_mate(k, j):
        block = latents.at[source_at(k, j), part]
        copy = send(block, block, lcs.at[k, j], lcr.at[k, j], sp, near)
        copy.start()
        tail.append(copy.wait_send)
        shares[k, j] = copy

    def latent_x(k, j):
        block = latents.at[sp, part]
        return send(block, block, lxs.at[k, j], lxr.at[k, j], turn_at(j), tp)

    for k in range(1, groups):
        lat_copies[k - 1].wait_recv()
        tail.append(lat_copies[k - 1].wait_send)
        block = latents.at[source_at(k, 0), part]
        for j in range(1, turns):
            copy = send(block, block, lxs.at[k, j], lxr.at[k, j], turn_at(j), tp)
            copy.start()
            tail.append(copy.wait_send)
        to_mate(k, 0)
    for m in range(2):
        pass_weights(m, 0)

    per = min(KEY_BLOCK // rows, count)
    blocks = count // per
    peaks[...] = jnp.full(peaks.shape, -jnp.inf, F32)
    tops[...] = jnp.full(tops.shape, -jnp.inf, F32)
    totals[...] = jnp.zeros(totals.shape, F32)
    sums[...] = jnp.zeros(sums.shape, F32)

    def score(shard, slot):
        rows_here = latents[shard, 0:rows, :]
        turned_here = latents[shard, rows : rows + ROPE, :]
        keys = across_dot(key_all[...], rows_here).astype(BF)
        vals[pl.ds(slot * rows, rows), :] = dot(rows_here, value_all[...]).astype(BF)
        for n, (query, plain, _, first_key, _) in enumerate(heads):
            joined = jnp.concatenate([keys[first_key : first_key + plain], turned_here], axis=0)
            scores = dot(query, joined)
            board[n, :, slot * rows : (slot + 1) * rows] = scores
            best = peaks[n]
            for c in range(0, rows, 128):
                best = jnp.maximum(best, scores[:, c : c + 128])
            peaks[n] = best

    def gather_softmax():
        for n, (_, plain, value_dim, _, first_value) in enumerate(heads):
            scale = (plain + ROPE) ** (-0.5) * 1.4426950408889634
            before = tops[n]
            largest = jnp.broadcast_to(jnp.max(peaks[n], axis=-1, keepdims=True), before.shape) * scale
            factor = jnp.exp2(before - largest)
            tops[n] = largest
            totals[n] = totals[n] * factor
            at_v = slice(first_value, first_value + value_dim)
            sums[:, at_v] = sums[:, at_v] * factor[:, 0:1]

            def tile(i, inner):
                at = pl.ds(pl.multiple_of(i * ROW_TILE, ROW_TILE), ROW_TILE)
                top = tops[n, at, :]
                total = totals[n, at, :]
                for c in range(0, per * rows, 128):
                    lifted = jnp.exp2(board[n, at, c : c + 128] * scale - top)
                    total = total + lifted
                    raised[at, c : c + 128] = lifted.astype(BF)
                totals[n, at, :] = total
                return inner

            lax.fori_loop(0, rows // ROW_TILE, tile, 0)
            sums[:, at_v] = sums[:, at_v] + dot(raised[...], vals[:, at_v])

    if blocks == 1:
        slot = 0
        score(sp, slot)
        for k in range(1, groups):
            shares[k, 0].wait_recv()
            slot += 1
            score(source_at(k, 0), slot)
        for k in range(groups):
            for j in range(1, turns):
                latent_x(k, j).wait_recv()
                to_mate(k, j)
        pass_weights(0, 1)
        for k in range(groups):
            for j in range(1, turns):
                shares[k, j].wait_recv()
                slot += 1
                score(source_at(k, j), slot)
        gather_softmax()
    else:
        for k in range(1, groups):
            shares[k, 0].wait_recv()
        for k in range(groups):
            for j in range(1, turns):
                latent_x(k, j).wait_recv()
                to_mate(k, j)
        pass_weights(0, 1)
        for k in range(groups):
            for j in range(1, turns):
                shares[k, j].wait_recv()

        def attend(b, carry):
            for s in range(per):
                score(b * per + s, s)
            gather_softmax()
            return carry

        lax.fori_loop(0, blocks, attend, 0)
    for n, (_, _, value_dim, _, first_value) in enumerate(heads):
        total = jnp.sum(totals[n], axis=-1, keepdims=True)
        result = (sums[:, first_value : first_value + value_dim] / total).astype(BF)
        if first_value < wide_v:
            for t in range(parts):
                place = t * wide_v + first_value

                @pl.when(tp == t)
                def _():
                    att_w[:, place : place + value_dim] = result
        else:
            place = first_value - wide_v
            att_n[tp, :, place : place + value_dim] = result

    rest = [
        share(
            att_w.at[:, pl.ds(pl.multiple_of(tp * wide_v, 128), wide_v)],
            lambda t: att_w.at[:, pl.ds(pl.multiple_of(t * wide_v, 128), wide_v)],
            3,
        ),
        share(att_n.at[tp], lambda t: att_n.at[t], 4),
    ]
    done = [step() for step in onward]
    for k in range(2, groups):
        pass_weights(0, k)
    done += [step() for step in rest]
    for step in done:
        step()
    for i in range(3, 6):
        loads[i].wait()
    for copy in gain_copies:
        copy.wait_recv()

    block_w = width // parts
    narrow = jnp.concatenate([att_n[t] for t in range(parts)], axis=1)
    run = jnp.zeros((rows, 128), F32)
    for c in range(parts):
        at = slice(c * block_w, (c + 1) * block_w)
        mixed = dot(att_w[...], out_w[:, at]) + dot(narrow, out_n[:, at])
        mixed = mixed + DEEP_ALPHA * res_all[c].astype(F32)
        board[0, :, at] = mixed
        for b in range(0, block_w, 128):
            run = run + mixed[:, b : b + 128]
    tops[0] = jnp.broadcast_to(jnp.sum(run, axis=-1, keepdims=True) / width, run.shape)

    def moments(i, inner):
        at = pl.ds(pl.multiple_of(i * ROW_TILE, ROW_TILE), ROW_TILE)
        center = tops[0, at, :]
        square = jnp.zeros(center.shape, F32)
        for c in range(0, width, 128):
            moved = board[0, at, c : c + 128] - center
            square = square + moved * moved
        totals[0, at, :] = square
        return inner

    lax.fori_loop(0, rows // ROW_TILE, moments, 0)
    spread = jnp.sum(totals[0], axis=-1, keepdims=True) / width
    totals[0] = jnp.broadcast_to(lax.rsqrt(spread + EPS_LAYER), totals.shape[1:])

    def first_norm(i, inner):
        at = pl.ds(pl.multiple_of(i * ROW_TILE, ROW_TILE), ROW_TILE)
        center, scale = tops[0, at, :], totals[0, at, :]
        for c in range(0, width, 128):
            t, b = c // block_w, c % block_w
            moved = (board[0, at, c : c + 128] - center) * scale
            moved = moved * gains[t, 0:1, b : b + 128] + gains[t, 1:2, b : b + 128]
            x_all[group, at, c : c + 128] = moved.astype(BF)
        return inner

    lax.fori_loop(0, rows // ROW_TILE, first_norm, 0)

    def strip(t):
        return pl.ds(pl.multiple_of(t * quarter, quarter), quarter)

    def ahead(source, step):
        block = x_all.at[source, strip(tp)]
        target = (group + step) * turns + turn
        return send(block, block, ags.at[source, (step + 1) // 2], agr.at[source], target, tp)

    def maybe(condition, act):
        @pl.when(condition)
        def _():
            act()

    for step in (1, -1):
        inside = (group + step >= 0) & (group + step < groups)
        maybe(inside, lambda step=step: ahead(group, step).start())
        tail.append(
            lambda inside=inside, step=step: maybe(inside, lambda: ahead(group, step).wait_send())
        )
    send_weights(2)
    pass_weights(2, 0)
    for k in range(1, groups):
        pass_weights(1, k)

    relayed = {}

    def relay(k):
        source = sources[k]
        ahead(source, 1).wait_recv()
        for step in (1, -1):
            from_behind = source < group if step == 1 else source > group
            inside = from_behind & (group + step >= 0) & (group + step < groups)
            maybe(inside, lambda step=step: ahead(source, step).start())
            tail.append(
                lambda inside=inside, step=step: maybe(
                    inside, lambda: ahead(source, step).wait_send()
                )
            )
        block = x_all.at[source, strip(tp)]
        for i, peer in ((0, far), (1, near)):
            copy = send(block, block, ars.at[k, i], arr.at[k, i], sp, peer)
            copy.start()
            tail.append(copy.wait_send)
            relayed[k, i] = copy

    def relay_far(k):
        relayed[k, 0].wait_recv()
        block = x_all.at[sources[k], strip(far)]
        copy = send(block, block, ars.at[k, 2], arr.at[k, 2], sp, near)
        copy.start()
        tail.append(copy.wait_send)
        relayed[k, 2] = copy

    def compute(k):
        if k:
            relayed[k, 1].wait_recv()
            relayed[k, 2].wait_recv()
        gate = jnp.zeros((rows, hidden_count), F32)
        lifted = gate
        for i in range(count):
            columns = x_all[sources[k], :, i * depth : (i + 1) * depth]
            gate += across_dot(columns, weights[0, i])
            lifted += across_dot(columns, weights[1, i])
        hidden[k] = (jax.nn.silu(gate) * lifted).astype(BF)

    span = turns * depth

    def column_group(c):
        return (group - c + groups) % groups

    firsts, seconds, thirds = {}, {}, {}

    def down(c, k):
        for j in range(turns):
            source = column_group(c) * turns + j
            product = dot(hidden[k], weights[2, source])
            parts_f[c, pl.ds(k * rows, rows), j * depth : (j + 1) * depth] = product
        for h in range(2):
            first = pl.multiple_of(k * rows + (2 * h + 1 - low) * quarter, quarter)
            s1[c, k, h] = parts_f[c, pl.ds(first, quarter), :].astype(BF)
        firsts[c, k] = send(s1.at[c, k], r1.at[c, k], p1s.at[c, k], p1r.at[c, k], sp, near)
        firsts[c, k].start()
        tail.append(firsts[c, k].wait_send)

    def second(c, k):
        firsts[c, k].wait_recv()
        first = pl.multiple_of(k * rows + (2 * (1 - high) + low) * quarter, quarter)
        kept = parts_f[c, pl.ds(first, quarter), :]
        s2[c, k] = (kept + r1[c, k, 1 - high].astype(F32)).astype(BF)
        seconds[c, k] = send(s2.at[c, k], r2.at[c, k], p2s.at[c, k], p2r.at[c, k], sp, far)
        seconds[c, k].start()
        tail.append(seconds[c, k].wait_send)

    def third(c, k):
        seconds[c, k].wait_recv()
        first = pl.multiple_of(k * rows + tp * quarter, quarter)
        total = parts_f[c, pl.ds(first, quarter), :]
        total = total + r1[c, k, high].astype(F32) + r2[c, k].astype(F32)
        if k == 0:
            parts_f[c, pl.ds(first, quarter), :] = total
        else:
            s3[c, k] = total.astype(BF)
            place = r3.at[column_group(c), group]
            copy = send(
                s3.at[c, k], place, p3s.at[c, k], p3r.at[column_group(c), group],
                sources[k] * turns + turn, tp,
            )
            copy.start()
            tail.append(copy.wait_send)

    for k in range(1, groups):
        relay(k)
        if k == 1:
            for m in range(2):
                for q in range(groups):
                    weights_here(m, q)
        compute(k - 1) if k == 1 else None
        relay_far(k)
        compute(k) if k < groups - 1 else None
    for k in range(1, groups):
        pass_weights(2, k)
    compute(groups - 1)

    units = [(c, k) for c in range(groups) for k in (list(range(1, groups)) + [0])]
    lag = groups
    for i in range(len(units) + 2 * lag):
        if i < len(units):
            c, k = units[i]
            if k == 1 or groups == 1:
                weights_here(2, c)
            down(c, k)
        if 0 <= i - lag < len(units):
            second(*units[i - lag])
        if 0 <= i - 2 * lag < len(units):
            third(*units[i - 2 * lag])

    def arrival(c, k):
        place = r3.at[column_group(c), sources[k]]
        return send(
            place, place, p3s.at[c, k], p3r.at[column_group(c), sources[k]], sp, near
        )

    for c in range(groups):
        for k in range(1, groups):
            arrival(c, k).wait_recv()
    gain2 = jnp.concatenate([gains[t, 2:3, :] for t in range(parts)], axis=1)
    bias2 = jnp.concatenate([gains[t, 3:4, :] for t in range(parts)], axis=1)
    for i in range(quarter // ROW_TILE):
        base = pl.multiple_of(tp * quarter + i * ROW_TILE, ROW_TILE)
        at = slice(i * ROW_TILE, (i + 1) * ROW_TILE)
        pieces = []
        for g in range(groups):
            total = parts_f[(group - g + groups) % groups, pl.ds(base, ROW_TILE), 0:span]
            for k in range(1, groups):
                total = total + r3[g, sources[k], at, :].astype(F32)
            pieces.append(total)
        total = jnp.concatenate(pieces, axis=1)
        total = total + DEEP_ALPHA * x_all[group, pl.ds(base, ROW_TILE), :].astype(F32)
        result = layer_norm(total, gain2, bias2).astype(BF)
        for c in range(parts):
            final[c, at, :] = result[:, c * block_w : (c + 1) * block_w]
    finals = []
    for i, peer in enumerate((far, diag, near)):
        copy = send(final.at[peer], out_ref.at[strip(tp)], fs.at[i], fr.at[i], sp, peer)
        copy.start()
        finals.append(copy)
    local = pltpu.make_async_copy(final.at[tp], out_ref.at[strip(tp)], fl)
    local.start()
    for copy in finals:
        copy.wait_recv()
        copy.wait_send()
    local.wait()
    for wait in tail:
        wait()


def whole_layer(args, constants, groups, turns, parts):
    (
        residual, query_latent, shared_latent, rotary_key, query_gain, latent_gain,
        query_narrow, key_narrow, value_narrow, query_wide, key_wide, value_wide,
        output_narrow, output_wide, first_gain, first_bias,
        gate_weight, up_weight, down_weight, second_gain, second_bias,
    ) = args
    count = groups * turns
    rows, own_width = residual.shape
    width = own_width * parts
    depth, hidden_local = gate_weight.shape
    hidden_count = hidden_local // groups
    heads_n, heads_w = key_narrow.shape[0] // NOPE_A, key_wide.shape[1] // NOPE_B
    heads = heads_n + heads_w
    quarter = rows // parts
    keys = min(KEY_BLOCK, count * rows)
    latent_width = shared_latent.shape[1]
    dma = pltpu.SemaphoreType.DMA
    vm, far_ref = pl.BlockSpec(memory_space=pltpu.VMEM), pl.BlockSpec(memory_space=pl.ANY)
    names = [vm] * 21
    for i in (0, 12, 13, 16, 17, 18):
        names[i] = far_ref
    strip = (quarter, turns * depth)
    return pl.pallas_call(
        functools.partial(layer_kernel, groups, turns, parts),
        out_shape=jax.ShapeDtypeStruct(residual.shape, BF),
        in_specs=names + [vm] * len(constants),
        out_specs=vm,
        scratch_shapes=[
            pltpu.VMEM((2, depth, hidden_local), BF),
            pltpu.VMEM((3, hidden_local, depth), BF),
            pltpu.VMEM((3, count, hidden_count, depth), BF),
            pltpu.VMEM((count, rows + ROPE, latent_width), BF),
            pltpu.VMEM((rows, ROPE), F32),
            pltpu.VMEM((rows, ROPE), F32),
            pltpu.VMEM((heads, rows, max(width, keys)), F32),
            pltpu.VMEM((groups, groups * rows, turns * depth), F32),
            pltpu.VMEM((rows, keys), BF),
            pltpu.VMEM((heads_w * NOPE_B + heads_n * NOPE_A, latent_width), BF),
            pltpu.VMEM((latent_width, heads_w * V_B + heads_n * V_A), BF),
            pltpu.VMEM((keys, heads_w * V_B + heads_n * V_A), BF),
            pltpu.VMEM((heads, rows, 128), F32),
            pltpu.VMEM((heads, rows, 128), F32),
            pltpu.VMEM((heads, rows, 128), F32),
            pltpu.VMEM((rows, heads_w * V_B + heads_n * V_A), F32),
            pltpu.VMEM((parts * heads_n * V_A, width), BF),
            pltpu.VMEM((parts * heads_w * V_B, width), BF),
            pltpu.VMEM((parts,) + residual.shape, BF),
            pltpu.VMEM((8, own_width), F32),
            pltpu.VMEM((parts, 8, own_width), F32),
            pltpu.VMEM((parts, rows, heads_n * V_A), BF),
            pltpu.VMEM((rows, parts * heads_w * V_B), BF),
            pltpu.VMEM((groups, rows, width), BF),
            pltpu.VMEM((groups, rows, hidden_count), BF),
            pltpu.VMEM((groups, groups, 2) + strip, BF),
            pltpu.VMEM((groups, groups, 2) + strip, BF),
            pltpu.VMEM((groups, groups) + strip, BF),
            pltpu.VMEM((groups, groups) + strip, BF),
            pltpu.VMEM((groups, groups) + strip, BF),
            pltpu.VMEM((groups, groups) + strip, BF),
            pltpu.VMEM((parts, quarter, own_width), BF),
            dma((6,)),
            dma((groups,)),
            dma((groups,)),
            dma((groups, turns)),
            dma((groups, turns)),
            dma((groups, turns)),
            dma((groups, turns)),
            dma((3, groups)),
            dma((3, groups)),
            dma((3, groups, turns)),
            dma((3, groups, turns)),
            dma((3,)),
            dma((5, 3)),
            dma((5, 3)),
            dma((3,)),
            dma((3,)),
            dma((groups, 2)),
            dma((groups,)),
            dma((groups, 3)),
            dma((groups, 3)),
            dma((groups, groups)),
            dma((groups, groups)),
            dma((groups, groups)),
            dma((groups, groups)),
            dma((groups, groups)),
            dma((groups, groups)),
            dma((3,)),
            dma((3,)),
            dma(()),
        ],
        compiler_params=pltpu.CompilerParams(
            collective_id=0, has_side_effects=True, vmem_limit_bytes=62 * 2**20
        ),
        name="layer",
    )(*args, *constants)


def body(*args):
    args = [a.reshape(1, -1) if a.ndim == 1 else a for a in args]
    for i in (3, 6, 7, 8, 9):
        args[i] = args[i].T
    rows, own_width = args[0].shape
    device_count, parts = lax.axis_size("sp"), lax.axis_size("tp")
    hidden_local = args[16].shape[1]
    groups = split_groups(device_count, hidden_local, own_width * parts, rows)
    turns = device_count // groups
    constants = [jnp.asarray(t) for t in axial_tables(rows * device_count)]
    constants.append(jnp.asarray(swap_matrix(), BF))
    return whole_layer(args, constants, groups, turns, parts)


def solution(mesh):
    return jax.shard_map(
        body,
        mesh=mesh,
        in_specs=(
            P("sp", "tp"),
            P("sp", None),
            P("sp", None),
            P("sp", None),
            P(),
            P(),
            P(None, "tp"),
            P(None, "tp"),
            P(None, "tp"),
            P(None, "tp"),
            P(None, "tp"),
            P(None, "tp"),
            P("tp", None),
            P("tp", None),
            P("tp"),
            P("tp"),
            P("sp", "tp"),
            P("sp", "tp"),
            P("tp", "sp"),
            P("tp"),
            P("tp"),
        ),
        out_specs=P("sp", "tp"),
        check_vma=False,
    )
```

```python
import functools

import jax
import jax.numpy as jnp
import numpy as np
from jax import lax
from jax.experimental import pallas as pl
from jax.experimental.pallas import tpu as pltpu
from jax.sharding import PartitionSpec as P

ROPE = 32
NOPE_A = 64
V_A = 64
NOPE_B = 128
V_B = 128
GRID_W = 64

EPS_ROOT = 1e-06
EPS_LAYER = 1e-05
THETA = 10000.0
DEEP_ALPHA = 2.0**0.25

KEY_BLOCK = 2048
ROW_TILE = 16
HELD = 3
MESH = pl.DeviceIdType.MESH
BF = jnp.bfloat16
F32 = jnp.float32


def axial_tables(row_total):
    quarter = ROPE // 4
    freqs = np.float32(THETA) ** (-(2.0 * np.arange(quarter, dtype=np.float32)) / (2 * quarter))
    freqs = freqs.astype(np.float32)

    def spread(count, first):
        angle = np.arange(count, dtype=np.float32)[:, None] * freqs
        out = []
        for fn in (np.cos, np.sin):
            table = np.zeros((count, ROPE), np.float32)
            wave = fn(angle).astype(np.float32)
            start = 0 if first else ROPE // 2
            table[:, start : start + quarter] = wave
            table[:, start + quarter : start + 2 * quarter] = wave
            out.append(table)
        return out

    return spread(row_total // GRID_W, True) + spread(GRID_W, False)


def swap_matrix():
    quarter = ROPE // 4
    swap = np.zeros((ROPE, ROPE), np.float32)
    for base in (0, ROPE // 2):
        for i in range(quarter):
            swap[base + i, base + quarter + i] = -1.0
            swap[base + quarter + i, base + i] = 1.0
    return swap


def split_groups(device_count, hidden_local, width, row_count):
    best = None
    for groups in range(1, device_count + 1):
        if device_count % groups or hidden_local % groups:
            continue
        moved = 3 * width * hidden_local // groups + 2 * row_count * groups * width
        if best is None or moved < best[0]:
            best = (moved, groups)
    return best[1]


def other(index, bit):
    return index + bit * (1 - 2 * ((index // bit) % 2))


def send(source, target, send_sem, recv_sem, sp, tp):
    return pltpu.make_async_remote_copy(
        src_ref=source,
        dst_ref=target,
        send_sem=send_sem,
        recv_sem=recv_sem,
        device_id={"sp": sp, "tp": tp},
        device_id_type=MESH,
    )


def dot(a, b):
    return jnp.dot(a, b, preferred_element_type=F32)


def across_dot(rows, columns):
    return lax.dot_general(
        rows, columns, (((1,), (1,)), ((), ())), preferred_element_type=F32
    )


def root_norm(values, gain):
    return values * lax.rsqrt(jnp.mean(values * values, axis=-1, keepdims=True) + EPS_ROOT) * gain


def layer_norm(values, gain, bias):
    center = jnp.mean(values, axis=-1, keepdims=True)
    moved = values - center
    spread = jnp.mean(moved * moved, axis=-1, keepdims=True)
    return moved * lax.rsqrt(spread + EPS_LAYER) * gain + bias


def chain_orders(groups):
    found = []
    for g in range(groups):
        outward = 1 if 2 * g >= groups else -1
        found.append(sorted(range(groups), key=lambda s: (abs(s - g), (g - s) * outward)))
    return found


def pick(index, options):
    value = options[-1]
    for i, option in enumerate(options[:-1]):
        value = jnp.where(index == i, option, value)
    return value


def layer_kernel(groups, turns, parts, staged_inputs, *refs):
    inputs, held, fetch_sem = refs[:26], refs[-1 - len(staged_inputs) : -1], refs[-1]
    fetches = []
    for i, place in enumerate(staged_inputs):
        fetch = pltpu.make_async_copy(inputs[place], held[i], fetch_sem.at[i])
        fetch.start()
        fetches.append(fetch)
        inputs = inputs[:place] + (held[i],) + inputs[place + 1 :]
    refs = refs[: -1 - len(staged_inputs)]
    (
        residual, query_latent, shared_latent, rotary_key, query_gain, latent_gain,
        query_narrow, key_narrow, value_narrow, query_wide, key_wide, value_wide,
        output_narrow, output_wide, first_gain, first_bias,
        gate_weight, up_weight, down_weight, second_gain, second_bias,
        row_cos, row_sin, col_cos, col_sin, swap,
    ) = inputs
    out_ref = refs[26]
    (
        raw, staged, weights, latents, cosine, sine, board, parts_f, raised, key_all, value_all, vals,
        peaks, tops, totals, sums, out_n, out_w, res_all, own_gains, gains,
        att_n, att_w, x_all, hidden, s1, r1, s2, r2, s3, r3, final,
    ) = refs[27:59]
    (
        load_sem, lzs, lzr, lxs, lxr, lcs, lcr, wzs, wzr, wxs, wxr, wls,
        tps, tpr, gns, gnr, ags, agr, ars, arr, p1s, p1r, p2s, p2r, p3s, p3r, fs, fr, fl,
    ) = refs[59:]
    sp, tp = lax.axis_index("sp"), lax.axis_index("tp")
    count = groups * turns
    group, turn = sp // turns, sp % turns
    low, high = tp % 2, tp // 2
    near, far = other(tp, 1), other(tp, 2)
    diag = other(far, 1)
    rows = query_latent.shape[0]
    width = residual.shape[1] * parts
    hidden_count, depth = weights.shape[2], weights.shape[3]
    quarter = rows // parts
    orders = chain_orders(groups)
    sources = [group] + [pick(group, [orders[g][k] for g in range(groups)]) for k in range(1, groups)]
    heads_w, heads_n = key_wide.shape[1] // NOPE_B, key_narrow.shape[0] // NOPE_A
    tail = []

    def group_at(k):
        return ((group + k) % groups) * turns + turn

    def turn_at(j):
        return group * turns + (turn + j) % turns

    def source_at(k, j):
        return ((group - k + groups) % groups) * turns + (turn - j + turns) % turns

    wide_v, narrow_v = heads_w * V_B, heads_n * V_A
    own_w = pl.ds(pl.multiple_of(tp * wide_v, 16), wide_v)
    own_n = pl.ds(pl.multiple_of(tp * narrow_v, 16), narrow_v)
    loads = []
    for i, (source, target) in enumerate(
        (
            (gate_weight, raw.at[0]),
            (up_weight, raw.at[1]),
            (down_weight, staged.at[2]),
            (output_narrow, out_n.at[own_n]),
            (output_wide, out_w.at[own_w]),
            (residual, res_all.at[tp]),
        )
    ):
        load = pltpu.make_async_copy(source, target, load_sem.at[i])
        load.start()
        loads.append(load)

    barrier = pltpu.get_barrier_semaphore()
    peers = [(group_at(k), tp) for k in range(1, groups)]
    peers += [(turn_at(j), tp) for j in range(1, turns)]
    peers += [(sp, near), (sp, far), (sp, diag)]
    for a, b in peers:
        pl.semaphore_signal(barrier, inc=1, device_id={"sp": a, "tp": b}, device_id_type=MESH)

    for fetch in fetches:
        fetch.wait()

    grid_rows = rows // GRID_W
    for i in range(grid_rows):
        at = pl.ds(i * GRID_W, GRID_W)
        line = pl.ds(sp * grid_rows + i, 1)
        cosine[at, :] = col_cos[...] + row_cos[line, :]
        sine[at, :] = col_sin[...] + row_sin[line, :]
    latents[sp, 0:rows, :] = root_norm(shared_latent[...].astype(F32), latent_gain[...]).astype(BF)
    rotary = rotary_key[...]
    turned = rotary.astype(F32) * cosine[...].T + dot(swap[...], rotary) * sine[...].T
    latents[sp, rows : rows + ROPE, :] = turned.astype(BF)
    own_gains[...] = jnp.zeros(own_gains.shape, F32)
    for i, ref in enumerate((first_gain, first_bias, second_gain, second_bias)):
        own_gains[i : i + 1, :] = ref[...]
        gains[tp, i : i + 1, :] = ref[...]
    pl.semaphore_wait(barrier, len(peers))

    half = (rows + ROPE) // 2
    part = pl.ds(pl.multiple_of(low * half, half), half)
    lat_copies = []
    for k in range(1, groups):
        block = latents.at[sp, part]
        copy = send(block, block, lzs.at[k], lzr.at[k], group_at(k), tp)
        copy.start()
        lat_copies.append(copy)
    for j in range(1, turns):
        block = latents.at[sp, part]
        copy = send(block, block, lxs.at[0, j], lxr.at[0, j], turn_at(j), tp)
        copy.start()
        tail.append(copy.wait_send)

    def share(source, view, i):
        a = send(source, view(tp), tps.at[i, 0], tpr.at[i, 0], sp, far)
        b = send(source, view(tp), tps.at[i, 1], tpr.at[i, 1], sp, near)
        a.start()
        b.start()
        tail.append(a.wait_send)
        tail.append(b.wait_send)

        def onward():
            a.wait_recv()
            c = send(view(far), view(far), tps.at[i, 2], tpr.at[i, 2], sp, near)
            c.start()
            tail.append(c.wait_send)

            def done():
                b.wait_recv()
                c.wait_recv()

            return done

        return onward

    onward = [
        share(output_wide, lambda t: out_w.at[pl.ds(pl.multiple_of(t * wide_v, 16), wide_v)], 0),
        share(output_narrow, lambda t: out_n.at[pl.ds(pl.multiple_of(t * narrow_v, 16), narrow_v)], 1),
        share(residual, lambda t: res_all.at[t], 2),
    ]
    gain_copies = []
    for i, peer in enumerate((near, far, diag)):
        copy = send(own_gains, gains.at[tp], gns.at[i], gnr.at[i], sp, peer)
        copy.start()
        gain_copies.append(copy)
        tail.append(copy.wait_send)

    loads[0].wait()
    staged[0] = raw[0].T
    loads[1].wait()
    staged[1] = raw[1].T
    loads[2].wait()

    def piece(m, k):
        first = pl.multiple_of(sources[k] * hidden_count, 16)
        return staged.at[m, pl.ds(first, hidden_count)]

    weight_z = {}

    def keep_weights(m):
        local = pltpu.make_async_copy(piece(m, 0), weights.at[m, sp], wls.at[m])
        local.start()
        weight_z[m, 0] = local

    def send_weights(m, started):
        for k in range(1, groups):
            target = sources[k] * turns + turn
            copy = send(piece(m, k), weights.at[m, sp], wzs.at[m, k], wzr.at[m, group], target, tp)
            if k <= started:
                copy.start()
            tail.append(copy.wait_send)
            weight_z[m, k] = copy

    weight_x = {}

    def pass_weights(m, k):
        source = sources[k] * turns + turn
        block = weights.at[m, source] if k else piece(m, 0)
        if k:
            send(block, block, wzs.at[m, k], wzr.at[m, sources[k]], sp, near).wait_recv()
        for j in range(1, turns):
            copy = send(block, weights.at[m, source], wxs.at[m, k, j], wxr.at[m, k, j], turn_at(j), tp)
            copy.start()
            tail.append(copy.wait_send)
            weight_x[m, k, j] = copy

    def weights_here(m, k):
        if k == 0:
            weight_z[m, 0].wait()
        for j in range(1, turns):
            weight_x[m, k, j].wait_recv()

    send_weights(0, groups)
    send_weights(1, HELD)
    for m in range(3):
        keep_weights(m)

    normed = root_norm(query_latent[...].astype(F32), query_gain[...]).astype(BF)
    heads = []
    for weight, plain, value_dim, head_count, first_key, first_value in (
        (query_wide, NOPE_B, V_B, heads_w, 0, 0),
        (query_narrow, NOPE_A, V_A, heads_n, heads_w * NOPE_B, wide_v),
    ):
        for h in range(head_count):
            first = h * (plain + ROPE)
            turn_w = weight[first + plain : first + plain + ROPE, :]
            plain_q = across_dot(normed, weight[first : first + plain, :]).astype(BF)
            turn_q = across_dot(normed, turn_w)
            flip_q = across_dot(normed, dot(swap[...], turn_w).astype(BF))
            turn_q = (turn_q * cosine[...] + flip_q * sine[...]).astype(BF)
            query = jnp.concatenate([plain_q, turn_q], axis=1)
            heads.append((query, plain, value_dim, first_key + h * plain, first_value + h * value_dim))
    key_all[0 : heads_w * NOPE_B, :] = key_wide[...].T
    key_all[heads_w * NOPE_B :, :] = key_narrow[...]
    value_all[:, 0:wide_v] = value_wide[...]
    value_all[:, wide_v:] = value_narrow[...].T

    shares = {}

    def to_mate(k, j):
        block = latents.at[source_at(k, j), part]
        copy = send(block, block, lcs.at[k, j], lcr.at[k, j], sp, near)
        copy.start()
        tail.append(copy.wait_send)
        shares[k, j] = copy

    def latent_x(k, j):
        block = latents.at[sp, part]
        return send(block, block, lxs.at[k, j], lxr.at[k, j], turn_at(j), tp)

    for k in range(1, groups):
        lat_copies[k - 1].wait_recv()
        tail.append(lat_copies[k - 1].wait_send)
        block = latents.at[source_at(k, 0), part]
        for j in range(1, turns):
            copy = send(block, block, lxs.at[k, j], lxr.at[k, j], turn_at(j), tp)
            copy.start()
            tail.append(copy.wait_send)
        to_mate(k, 0)
    for m in range(3):
        pass_weights(m, 0)

    per = min(KEY_BLOCK // rows, count)
    blocks = count // per
    peaks[...] = jnp.full(peaks.shape, -jnp.inf, F32)
    tops[...] = jnp.full(tops.shape, -jnp.inf, F32)
    totals[...] = jnp.zeros(totals.shape, F32)
    sums[...] = jnp.zeros(sums.shape, F32)

    def score(shard, slot):
        rows_here = latents[shard, 0:rows, :]
        turned_here = latents[shard, rows : rows + ROPE, :]
        keys = across_dot(key_all[...], rows_here).astype(BF)
        vals[pl.ds(slot * rows, rows), :] = dot(rows_here, value_all[...]).astype(BF)
        for n, (query, plain, _, first_key, _) in enumerate(heads):
            joined = jnp.concatenate([keys[first_key : first_key + plain], turned_here], axis=0)
            scores = dot(query, joined)
            board[n, :, slot * rows : (slot + 1) * rows] = scores
            best = peaks[n]
            for c in range(0, rows, 128):
                best = jnp.maximum(best, scores[:, c : c + 128])
            peaks[n] = best

    def gather_softmax():
        for n, (_, plain, value_dim, _, first_value) in enumerate(heads):
            scale = (plain + ROPE) ** (-0.5) * 1.4426950408889634
            before = tops[n]
            largest = jnp.broadcast_to(jnp.max(peaks[n], axis=-1, keepdims=True), before.shape) * scale
            factor = jnp.exp2(before - largest)
            tops[n] = largest
            totals[n] = totals[n] * factor
            at_v = slice(first_value, first_value + value_dim)
            sums[:, at_v] = sums[:, at_v] * factor[:, 0:1]

            def tile(i, inner):
                at = pl.ds(pl.multiple_of(i * ROW_TILE, ROW_TILE), ROW_TILE)
                top = tops[n, at, :]
                total = totals[n, at, :]
                for c in range(0, per * rows, 128):
                    lifted = jnp.exp2(board[n, at, c : c + 128] * scale - top)
                    total = total + lifted
                    raised[at, c : c + 128] = lifted.astype(BF)
                totals[n, at, :] = total
                return inner

            lax.fori_loop(0, rows // ROW_TILE, tile, 0)
            sums[:, at_v] = sums[:, at_v] + dot(raised[...], vals[:, at_v])

    if blocks == 1:
        slot = 0
        score(sp, slot)
        for k in range(1, groups):
            shares[k, 0].wait_recv()
            slot += 1
            score(source_at(k, 0), slot)
        for k in range(groups):
            for j in range(1, turns):
                latent_x(k, j).wait_recv()
                to_mate(k, j)
        pass_weights(0, 1)
        for k in range(groups):
            for j in range(1, turns):
                shares[k, j].wait_recv()
                slot += 1
                score(source_at(k, j), slot)
        gather_softmax()
    else:
        for k in range(1, groups):
            shares[k, 0].wait_recv()
        for k in range(groups):
            for j in range(1, turns):
                latent_x(k, j).wait_recv()
                to_mate(k, j)
        pass_weights(0, 1)
        for k in range(groups):
            for j in range(1, turns):
                shares[k, j].wait_recv()

        def attend(b, carry):
            for s in range(per):
                score(b * per + s, s)
            gather_softmax()
            return carry

        lax.fori_loop(0, blocks, attend, 0)
    for n, (_, _, value_dim, _, first_value) in enumerate(heads):
        total = jnp.sum(totals[n], axis=-1, keepdims=True)
        result = (sums[:, first_value : first_value + value_dim] / total).astype(BF)
        if first_value < wide_v:
            for t in range(parts):
                place = t * wide_v + first_value

                @pl.when(tp == t)
                def _():
                    att_w[:, place : place + value_dim] = result
        else:
            place = first_value - wide_v
            att_n[tp, :, place : place + value_dim] = result

    rest = [
        share(
            att_w.at[:, pl.ds(pl.multiple_of(tp * wide_v, 128), wide_v)],
            lambda t: att_w.at[:, pl.ds(pl.multiple_of(t * wide_v, 128), wide_v)],
            3,
        ),
        share(att_n.at[tp], lambda t: att_n.at[t], 4),
    ]
    done = [step() for step in onward]
    done += [step() for step in rest]
    for step in done:
        step()
    for i in range(3, 6):
        loads[i].wait()
    for copy in gain_copies:
        copy.wait_recv()

    block_w = width // parts
    narrow = jnp.concatenate([att_n[t] for t in range(parts)], axis=1)
    run = jnp.zeros((rows, 128), F32)
    for c in range(parts):
        at = slice(c * block_w, (c + 1) * block_w)
        mixed = dot(att_w[...], out_w[:, at]) + dot(narrow, out_n[:, at])
        mixed = mixed + DEEP_ALPHA * res_all[c].astype(F32)
        board[0, :, at] = mixed
        for b in range(0, block_w, 128):
            run = run + mixed[:, b : b + 128]
    tops[0] = jnp.broadcast_to(jnp.sum(run, axis=-1, keepdims=True) / width, run.shape)

    def moments(i, inner):
        at = pl.ds(pl.multiple_of(i * ROW_TILE, ROW_TILE), ROW_TILE)
        center = tops[0, at, :]
        square = jnp.zeros(center.shape, F32)
        for c in range(0, width, 128):
            moved = board[0, at, c : c + 128] - center
            square = square + moved * moved
        totals[0, at, :] = square
        return inner

    lax.fori_loop(0, rows // ROW_TILE, moments, 0)
    spread = jnp.sum(totals[0], axis=-1, keepdims=True) / width
    totals[0] = jnp.broadcast_to(lax.rsqrt(spread + EPS_LAYER), totals.shape[1:])

    def first_norm(i, inner):
        at = pl.ds(pl.multiple_of(i * ROW_TILE, ROW_TILE), ROW_TILE)
        center, scale = tops[0, at, :], totals[0, at, :]
        for c in range(0, width, 128):
            t, b = c // block_w, c % block_w
            moved = (board[0, at, c : c + 128] - center) * scale
            moved = moved * gains[t, 0:1, b : b + 128] + gains[t, 1:2, b : b + 128]
            x_all[group, at, c : c + 128] = moved.astype(BF)
        return inner

    lax.fori_loop(0, rows // ROW_TILE, first_norm, 0)

    def strip(t):
        return pl.ds(pl.multiple_of(t * quarter, quarter), quarter)

    def ahead(source, step):
        block = x_all.at[source, strip(tp)]
        target = (group + step) * turns + turn
        return send(block, block, ags.at[source, (step + 1) // 2], agr.at[source], target, tp)

    def maybe(condition, act):
        @pl.when(condition)
        def _():
            act()

    for step in (1, -1):
        inside = (group + step >= 0) & (group + step < groups)
        maybe(inside, lambda step=step: ahead(group, step).start())
        tail.append(
            lambda inside=inside, step=step: maybe(inside, lambda: ahead(group, step).wait_send())
        )
    for k in range(HELD + 1, groups):
        weight_z[1, k].start()
    send_weights(2, 0)

    def start_down(first=1, past=groups):
        for k in range(first, past):
            weight_z[2, k].start()

    start_down(1, 2)
    for k in range(2, groups):
        pass_weights(0, k)
    for k in range(1, groups - 1):
        pass_weights(1, k)

    relayed = {}
    edge = (group == 0) | (group == groups - 1)

    def relay(k, only=None):
        source = sources[k]
        block = x_all.at[source, strip(tp)]
        steps = []
        for step in (1, -1):
            from_behind = source < group if step == 1 else source > group
            inside = from_behind & (group + step >= 0) & (group + step < groups)
            steps.append((inside, ahead(source, step)))
        if (k, 0) not in relayed:
            for i, peer in ((0, far), (1, near)):
                copy = send(block, block, ars.at[k, i], arr.at[k, i], sp, peer)
                tail.append(copy.wait_send)
                relayed[k, i] = copy
            for inside, copy in steps:
                tail.append(lambda inside=inside, copy=copy: maybe(inside, copy.wait_send))

        def act():
            steps[0][1].wait_recv()
            for inside, copy in steps:
                maybe(inside, copy.start)
            for i in range(2):
                relayed[k, i].start()

        if only is None:
            act()
        else:
            maybe(only, act)

    def relay_far(k):
        relayed[k, 0].wait_recv()
        block = x_all.at[sources[k], strip(far)]
        copy = send(block, block, ars.at[k, 2], arr.at[k, 2], sp, near)
        copy.start()
        tail.append(copy.wait_send)
        relayed[k, 2] = copy

    def compute(k):
        if k:
            relayed[k, 1].wait_recv()
            relayed[k, 2].wait_recv()
        gate = jnp.zeros((rows, hidden_count), F32)
        lifted = gate
        for i in range(count):
            columns = x_all[sources[k], :, i * depth : (i + 1) * depth]
            gate += across_dot(columns, weights[0, i])
            lifted += across_dot(columns, weights[1, i])
        hidden[k] = (jax.nn.silu(gate) * lifted).astype(BF)

    span = turns * depth

    def column_group(c):
        return sources[c]

    firsts, seconds, thirds = {}, {}, {}

    def down(c, k):
        for j in range(turns):
            source = column_group(c) * turns + j
            product = dot(hidden[k], weights[2, source])
            parts_f[column_group(c), pl.ds(k * rows, rows), j * depth : (j + 1) * depth] = product
        for h in range(2):
            first = pl.multiple_of(k * rows + (2 * h + 1 - low) * quarter, quarter)
            s1[c, k, h] = parts_f[column_group(c), pl.ds(first, quarter), :].astype(BF)
        firsts[c, k] = send(s1.at[c, k], r1.at[c, k], p1s.at[c, k], p1r.at[c, k], sp, near)
        firsts[c, k].start()
        tail.append(firsts[c, k].wait_send)

    def second(c, k):
        firsts[c, k].wait_recv()
        first = pl.multiple_of(k * rows + (2 * (1 - high) + low) * quarter, quarter)
        kept = parts_f[column_group(c), pl.ds(first, quarter), :]
        s2[c, k] = (kept + r1[c, k, 1 - high].astype(F32)).astype(BF)
        seconds[c, k] = send(s2.at[c, k], r2.at[c, k], p2s.at[c, k], p2r.at[c, k], sp, far)
        seconds[c, k].start()
        tail.append(seconds[c, k].wait_send)

    def third(c, k):
        seconds[c, k].wait_recv()
        first = pl.multiple_of(k * rows + tp * quarter, quarter)
        total = parts_f[column_group(c), pl.ds(first, quarter), :]
        total = total + r1[c, k, high].astype(F32) + r2[c, k].astype(F32)
        if k == 0:
            parts_f[column_group(c), pl.ds(first, quarter), :] = total
        else:
            s3[c, k] = total.astype(BF)
            place = r3.at[column_group(c), group]
            copy = send(
                s3.at[c, k], place, p3s.at[c, k], p3r.at[column_group(c), group],
                sources[k] * turns + turn, tp,
            )
            copy.start()
            tail.append(copy.wait_send)

    waiting, moving = [], []

    def push_second(left):
        while len(waiting) > left:
            second(*waiting[0])
            moving.append(waiting.pop(0))

    def push_third(left):
        while len(moving) > left:
            third(*moving.pop(0))

    def unit(c, k):
        down(c, k)
        waiting.append((c, k))
        push_second(2)
        push_third(6)

    last = groups - 1
    for k in range(1, last):
        relay(k)
        if k == 1:
            pass_weights(1, last)
    maybe(edge, lambda: start_down(2, max(last, 2)))
    if last > 1:
        relay_far(1)
    if last > 0:
        relay(last, ~edge)
    maybe(~edge, lambda: start_down(2, max(last, 2)))
    if last == 1:
        pass_weights(1, last)
    if last > 0:
        pass_weights(2, 1)
    for m in range(2):
        for q in range(groups):
            weights_here(m, q)
    compute(0)
    if last > 1:
        compute(1)
    start_down(max(last, 2))
    weights_here(2, 0)
    early = [*range(1, last), 0]
    for k in early[:1] + early[-1:] + early[1:-1] if last > 1 else [0]:
        if k > 1:
            relay_far(k)
            compute(k)
        unit(0, k)
    push_second(0)
    if last > 0:
        relay(last, edge)
        weights_here(2, 1)
        for k in early:
            unit(1, k)
        push_second(0)
        for c in range(2, groups):
            pass_weights(2, c)
        push_third(3)
        relay_far(last)
    for c in range(2, groups):
        weights_here(2, c)
        if c > 2:
            unit(c, last)
        for k in early:
            unit(c, k)
        if c == 2:
            compute(last)
            for b in range(3):
                unit(b, last)
    if last in (1, 2):
        compute(last)
        for c in range(groups):
            unit(c, last)
    push_second(0)
    push_third(0)

    def arrival(c, k):
        place = r3.at[column_group(c), sources[k]]
        return send(
            place, place, p3s.at[c, k], p3r.at[column_group(c), sources[k]], sp, near
        )

    for c in range(groups):
        for k in range(1, groups):
            arrival(c, k).wait_recv()
    gain2 = jnp.concatenate([gains[t, 2:3, :] for t in range(parts)], axis=1)
    bias2 = jnp.concatenate([gains[t, 3:4, :] for t in range(parts)], axis=1)
    for i in range(quarter // ROW_TILE):
        base = pl.multiple_of(tp * quarter + i * ROW_TILE, ROW_TILE)
        at = slice(i * ROW_TILE, (i + 1) * ROW_TILE)
        pieces = []
        for g in range(groups):
            total = parts_f[g, pl.ds(base, ROW_TILE), :]
            for k in range(1, groups):
                total = total + r3[g, sources[k], at, :].astype(F32)
            pieces.append(total)
        total = jnp.concatenate(pieces, axis=1)
        total = total + DEEP_ALPHA * x_all[group, pl.ds(base, ROW_TILE), :].astype(F32)
        result = layer_norm(total, gain2, bias2).astype(BF)
        for c in range(parts):
            final[c, at, :] = result[:, c * block_w : (c + 1) * block_w]
    finals = []
    for i, peer in enumerate((far, diag, near)):
        copy = send(final.at[peer], out_ref.at[strip(tp)], fs.at[i], fr.at[i], sp, peer)
        copy.start()
        finals.append(copy)
    local = pltpu.make_async_copy(final.at[tp], out_ref.at[strip(tp)], fl)
    local.start()
    for copy in finals:
        copy.wait_recv()
        copy.wait_send()
    local.wait()
    for wait in tail:
        wait()


def whole_layer(args, constants, groups, turns, parts):
    (
        residual, query_latent, shared_latent, rotary_key, query_gain, latent_gain,
        query_narrow, key_narrow, value_narrow, query_wide, key_wide, value_wide,
        output_narrow, output_wide, first_gain, first_bias,
        gate_weight, up_weight, down_weight, second_gain, second_bias,
    ) = args
    count = groups * turns
    rows, own_width = residual.shape
    width = own_width * parts
    depth, hidden_local = gate_weight.shape
    hidden_count = hidden_local // groups
    heads_n, heads_w = key_narrow.shape[0] // NOPE_A, key_wide.shape[1] // NOPE_B
    heads = heads_n + heads_w
    quarter = rows // parts
    keys = min(KEY_BLOCK, count * rows)
    latent_width = shared_latent.shape[1]
    dma = pltpu.SemaphoreType.DMA
    far_ref = pl.BlockSpec(memory_space=pl.ANY)
    operands = [*args, *constants]
    staged_inputs = [i for i in range(len(operands)) if i not in (0, 12, 13, 16, 17, 18)]
    strip = (quarter, turns * depth)
    return pl.pallas_call(
        functools.partial(layer_kernel, groups, turns, parts, staged_inputs),
        out_shape=jax.ShapeDtypeStruct(residual.shape, BF),
        in_specs=[far_ref] * len(operands),
        out_specs=far_ref,
        scratch_shapes=[
            pltpu.VMEM((2, depth, hidden_local), BF),
            pltpu.VMEM((3, hidden_local, depth), BF),
            pltpu.VMEM((3, count, hidden_count, depth), BF),
            pltpu.VMEM((count, rows + ROPE, latent_width), BF),
            pltpu.VMEM((rows, ROPE), F32),
            pltpu.VMEM((rows, ROPE), F32),
            pltpu.VMEM((heads, rows, max(width, keys)), F32),
            pltpu.VMEM((groups, groups * rows, turns * depth), F32),
            pltpu.VMEM((rows, keys), BF),
            pltpu.VMEM((heads_w * NOPE_B + heads_n * NOPE_A, latent_width), BF),
            pltpu.VMEM((latent_width, heads_w * V_B + heads_n * V_A), BF),
            pltpu.VMEM((keys, heads_w * V_B + heads_n * V_A), BF),
            pltpu.VMEM((heads, rows, 128), F32),
            pltpu.VMEM((heads, rows, 128), F32),
            pltpu.VMEM((heads, rows, 128), F32),
            pltpu.VMEM((rows, heads_w * V_B + heads_n * V_A), F32),
            pltpu.VMEM((parts * heads_n * V_A, width), BF),
            pltpu.VMEM((parts * heads_w * V_B, width), BF),
            pltpu.VMEM((parts,) + residual.shape, BF),
            pltpu.VMEM((8, own_width), F32),
            pltpu.VMEM((parts, 8, own_width), F32),
            pltpu.VMEM((parts, rows, heads_n * V_A), BF),
            pltpu.VMEM((rows, parts * heads_w * V_B), BF),
            pltpu.VMEM((groups, rows, width), BF),
            pltpu.VMEM((groups, rows, hidden_count), BF),
            pltpu.VMEM((groups, groups, 2) + strip, BF),
            pltpu.VMEM((groups, groups, 2) + strip, BF),
            pltpu.VMEM((groups, groups) + strip, BF),
            pltpu.VMEM((groups, groups) + strip, BF),
            pltpu.VMEM((groups, groups) + strip, BF),
            pltpu.VMEM((groups, groups) + strip, BF),
            pltpu.VMEM((parts, quarter, own_width), BF),
            dma((6,)),
            dma((groups,)),
            dma((groups,)),
            dma((groups, turns)),
            dma((groups, turns)),
            dma((groups, turns)),
            dma((groups, turns)),
            dma((3, groups)),
            dma((3, groups)),
            dma((3, groups, turns)),
            dma((3, groups, turns)),
            dma((3,)),
            dma((5, 3)),
            dma((5, 3)),
            dma((3,)),
            dma((3,)),
            dma((groups, 2)),
            dma((groups,)),
            dma((groups, 3)),
            dma((groups, 3)),
            dma((groups, groups)),
            dma((groups, groups)),
            dma((groups, groups)),
            dma((groups, groups)),
            dma((groups, groups)),
            dma((groups, groups)),
            dma((3,)),
            dma((3,)),
            dma(()),
            *[pltpu.VMEM(operands[i].shape, operands[i].dtype) for i in staged_inputs],
            dma((len(staged_inputs),)),
        ],
        compiler_params=pltpu.CompilerParams(
            collective_id=0, has_side_effects=True, vmem_limit_bytes=62 * 2**20
        ),
        name="layer",
    )(*operands)


def body(*args):
    args = [a.reshape(1, -1) if a.ndim == 1 else a for a in args]
    for i in (3, 6, 7, 8, 9):
        args[i] = args[i].T
    rows, own_width = args[0].shape
    device_count, parts = lax.axis_size("sp"), lax.axis_size("tp")
    hidden_local = args[16].shape[1]
    groups = split_groups(device_count, hidden_local, own_width * parts, rows)
    turns = device_count // groups
    constants = [jnp.asarray(t) for t in axial_tables(rows * device_count)]
    constants.append(jnp.asarray(swap_matrix(), BF))
    return whole_layer(args, constants, groups, turns, parts)


def solution(mesh):
    return jax.shard_map(
        body,
        mesh=mesh,
        in_specs=(
            P("sp", "tp"),
            P("sp", None),
            P("sp", None),
            P("sp", None),
            P(),
            P(),
            P(None, "tp"),
            P(None, "tp"),
            P(None, "tp"),
            P(None, "tp"),
            P(None, "tp"),
            P(None, "tp"),
            P("tp", None),
            P("tp", None),
            P("tp"),
            P("tp"),
            P("sp", "tp"),
            P("sp", "tp"),
            P("tp", "sp"),
            P("tp"),
            P("tp"),
        ),
        out_specs=P("sp", "tp"),
        check_vma=False,
    )
```

```python
import functools

import jax
import jax.numpy as jnp
import numpy as np
from jax import lax
from jax.experimental import pallas as pl
from jax.experimental.pallas import tpu as pltpu
from jax.sharding import PartitionSpec as P

ROPE = 32
NOPE_A = 64
V_A = 64
NOPE_B = 128
V_B = 128
GRID_W = 64

EPS_ROOT = 1e-06
EPS_LAYER = 1e-05
THETA = 10000.0
DEEP_ALPHA = 2.0**0.25

KEY_BLOCK = 2048
ROW_TILE = 16
HELD = 3
MESH = pl.DeviceIdType.MESH
BF = jnp.bfloat16
F32 = jnp.float32


def axial_tables(row_total):
    quarter = ROPE // 4
    freqs = np.float32(THETA) ** (-(2.0 * np.arange(quarter, dtype=np.float32)) / (2 * quarter))
    freqs = freqs.astype(np.float32)

    def spread(count, first):
        angle = np.arange(count, dtype=np.float32)[:, None] * freqs
        out = []
        for fn in (np.cos, np.sin):
            table = np.zeros((count, ROPE), np.float32)
            wave = fn(angle).astype(np.float32)
            start = 0 if first else ROPE // 2
            table[:, start : start + quarter] = wave
            table[:, start + quarter : start + 2 * quarter] = wave
            out.append(table)
        return out

    return spread(row_total // GRID_W, True) + spread(GRID_W, False)


def swap_matrix():
    quarter = ROPE // 4
    swap = np.zeros((ROPE, ROPE), np.float32)
    for base in (0, ROPE // 2):
        for i in range(quarter):
            swap[base + i, base + quarter + i] = -1.0
            swap[base + quarter + i, base + i] = 1.0
    return swap


def split_groups(device_count, hidden_local, width, row_count):
    best = None
    for groups in range(1, device_count + 1):
        if device_count % groups or hidden_local % groups:
            continue
        moved = 3 * width * hidden_local // groups + 2 * row_count * groups * width
        if best is None or moved < best[0]:
            best = (moved, groups)
    return best[1]


def other(index, bit):
    return index + bit * (1 - 2 * ((index // bit) % 2))


def send(source, target, send_sem, recv_sem, sp, tp):
    return pltpu.make_async_remote_copy(
        src_ref=source,
        dst_ref=target,
        send_sem=send_sem,
        recv_sem=recv_sem,
        device_id={"sp": sp, "tp": tp},
        device_id_type=MESH,
    )


def dot(a, b):
    return jnp.dot(a, b, preferred_element_type=F32)


def across_dot(rows, columns):
    return lax.dot_general(
        rows, columns, (((1,), (1,)), ((), ())), preferred_element_type=F32
    )


def root_norm(values, gain):
    return values * lax.rsqrt(jnp.mean(values * values, axis=-1, keepdims=True) + EPS_ROOT) * gain


def layer_norm(values, gain, bias):
    center = jnp.mean(values, axis=-1, keepdims=True)
    moved = values - center
    spread = jnp.mean(moved * moved, axis=-1, keepdims=True)
    return moved * lax.rsqrt(spread + EPS_LAYER) * gain + bias


def chain_orders(groups):
    found = []
    for g in range(groups):
        outward = 1 if 2 * g >= groups else -1
        found.append(sorted(range(groups), key=lambda s: (abs(s - g), (g - s) * outward)))
    return found


def pick(index, options):
    value = options[-1]
    for i, option in enumerate(options[:-1]):
        value = jnp.where(index == i, option, value)
    return value


def layer_kernel(groups, turns, parts, staged_inputs, *refs):
    inputs, held, fetch_sem = refs[:26], refs[-1 - len(staged_inputs) : -1], refs[-1]
    fetches = []
    for i, place in enumerate(staged_inputs):
        fetch = pltpu.make_async_copy(inputs[place], held[i], fetch_sem.at[i])
        fetch.start()
        fetches.append(fetch)
        inputs = inputs[:place] + (held[i],) + inputs[place + 1 :]
    refs = refs[: -1 - len(staged_inputs)]
    (
        residual, query_latent, shared_latent, rotary_key, query_gain, latent_gain,
        query_narrow, key_narrow, value_narrow, query_wide, key_wide, value_wide,
        output_narrow, output_wide, first_gain, first_bias,
        gate_weight, up_weight, down_weight, second_gain, second_bias,
        row_cos, row_sin, col_cos, col_sin, swap,
    ) = inputs
    out_ref = refs[26]
    (
        raw, staged, weights, latents, cosine, sine, board, parts_f, raised, key_all, value_all, vals,
        peaks, tops, totals, sums, out_n, out_w, res_all, own_gains, gains,
        att_n, att_w, x_all, hidden, s1, r1, s2, r2, s3, r3, final,
    ) = refs[27:59]
    (
        load_sem, lzs, lzr, lxs, lxr, lcs, lcr, wzs, wzr, wxs, wxr, wls,
        tps, tpr, gns, gnr, ags, agr, ars, arr, p1s, p1r, p2s, p2r, p3s, p3r, fs, fr, fl,
    ) = refs[59:]
    sp, tp = lax.axis_index("sp"), lax.axis_index("tp")
    count = groups * turns
    group, turn = sp // turns, sp % turns
    low, high = tp % 2, tp // 2
    near, far = other(tp, 1), other(tp, 2)
    diag = other(far, 1)
    rows = query_latent.shape[0]
    width = residual.shape[1] * parts
    hidden_count, depth = weights.shape[2], weights.shape[3]
    quarter = rows // parts
    orders = chain_orders(groups)
    sources = [group] + [pick(group, [orders[g][k] for g in range(groups)]) for k in range(1, groups)]
    heads_w, heads_n = key_wide.shape[1] // NOPE_B, key_narrow.shape[0] // NOPE_A
    tail = []

    def group_at(k):
        return ((group + k) % groups) * turns + turn

    def turn_at(j):
        return group * turns + (turn + j) % turns

    def source_at(k, j):
        return ((group - k + groups) % groups) * turns + (turn - j + turns) % turns

    wide_v, narrow_v = heads_w * V_B, heads_n * V_A
    own_w = pl.ds(pl.multiple_of(tp * wide_v, 16), wide_v)
    own_n = pl.ds(pl.multiple_of(tp * narrow_v, 16), narrow_v)
    loads = []
    for i, (source, target) in enumerate(
        (
            (gate_weight, raw.at[0]),
            (up_weight, raw.at[1]),
            (down_weight, staged.at[2]),
            (output_narrow, out_n.at[own_n]),
            (output_wide, out_w.at[own_w]),
            (residual, res_all.at[tp]),
        )
    ):
        load = pltpu.make_async_copy(source, target, load_sem.at[i])
        load.start()
        loads.append(load)

    barrier = pltpu.get_barrier_semaphore()
    peers = [(group_at(k), tp) for k in range(1, groups)]
    peers += [(turn_at(j), tp) for j in range(1, turns)]
    peers += [(sp, near), (sp, far), (sp, diag)]
    for a, b in peers:
        pl.semaphore_signal(barrier, inc=1, device_id={"sp": a, "tp": b}, device_id_type=MESH)

    for fetch in fetches:
        fetch.wait()

    grid_rows = rows // GRID_W
    for i in range(grid_rows):
        at = pl.ds(i * GRID_W, GRID_W)
        line = pl.ds(sp * grid_rows + i, 1)
        cosine[at, :] = col_cos[...] + row_cos[line, :]
        sine[at, :] = col_sin[...] + row_sin[line, :]
    latents[sp, 0:rows, :] = root_norm(shared_latent[...].astype(F32), latent_gain[...]).astype(BF)
    rotary = rotary_key[...]
    turned = rotary.astype(F32) * cosine[...].T + dot(swap[...], rotary) * sine[...].T
    latents[sp, rows : rows + ROPE, :] = turned.astype(BF)
    own_gains[...] = jnp.zeros(own_gains.shape, F32)
    for i, ref in enumerate((first_gain, first_bias, second_gain, second_bias)):
        own_gains[i : i + 1, :] = ref[...]
        gains[tp, i : i + 1, :] = ref[...]
    pl.semaphore_wait(barrier, len(peers))

    half = (rows + ROPE) // 2
    part = pl.ds(pl.multiple_of(low * half, half), half)
    lat_copies = []
    for k in range(1, groups):
        block = latents.at[sp, part]
        copy = send(block, block, lzs.at[k], lzr.at[k], group_at(k), tp)
        copy.start()
        lat_copies.append(copy)
    for j in range(1, turns):
        block = latents.at[sp, part]
        copy = send(block, block, lxs.at[0, j], lxr.at[0, j], turn_at(j), tp)
        copy.start()
        tail.append(copy.wait_send)

    def share(source, view, i):
        a = send(source, view(tp), tps.at[i, 0], tpr.at[i, 0], sp, far)
        b = send(source, view(tp), tps.at[i, 1], tpr.at[i, 1], sp, near)
        a.start()
        b.start()
        tail.append(a.wait_send)
        tail.append(b.wait_send)

        def onward():
            a.wait_recv()
            c = send(view(far), view(far), tps.at[i, 2], tpr.at[i, 2], sp, near)
            c.start()
            tail.append(c.wait_send)

            def done():
                b.wait_recv()
                c.wait_recv()

            return done

        return onward

    onward = [
        share(output_wide, lambda t: out_w.at[pl.ds(pl.multiple_of(t * wide_v, 16), wide_v)], 0),
        share(output_narrow, lambda t: out_n.at[pl.ds(pl.multiple_of(t * narrow_v, 16), narrow_v)], 1),
        share(residual, lambda t: res_all.at[t], 2),
    ]
    gain_copies = []
    for i, peer in enumerate((near, far, diag)):
        copy = send(own_gains, gains.at[tp], gns.at[i], gnr.at[i], sp, peer)
        copy.start()
        gain_copies.append(copy)
        tail.append(copy.wait_send)

    loads[0].wait()
    staged[0] = raw[0].T
    loads[1].wait()
    staged[1] = raw[1].T
    loads[2].wait()

    def piece(m, k):
        first = pl.multiple_of(sources[k] * hidden_count, 16)
        return staged.at[m, pl.ds(first, hidden_count)]

    weight_z = {}

    def keep_weights(m):
        local = pltpu.make_async_copy(piece(m, 0), weights.at[m, sp], wls.at[m])
        local.start()
        weight_z[m, 0] = local

    def send_weights(m, started):
        for k in range(1, groups):
            target = sources[k] * turns + turn
            copy = send(piece(m, k), weights.at[m, sp], wzs.at[m, k], wzr.at[m, group], target, tp)
            if k <= started:
                copy.start()
            tail.append(copy.wait_send)
            weight_z[m, k] = copy

    weight_x = {}

    def pass_weights(m, k):
        source = sources[k] * turns + turn
        block = weights.at[m, source] if k else piece(m, 0)
        if k:
            send(block, block, wzs.at[m, k], wzr.at[m, sources[k]], sp, near).wait_recv()
        for j in range(1, turns):
            copy = send(block, weights.at[m, source], wxs.at[m, k, j], wxr.at[m, k, j], turn_at(j), tp)
            copy.start()
            tail.append(copy.wait_send)
            weight_x[m, k, j] = copy

    def weights_here(m, k):
        if k == 0:
            weight_z[m, 0].wait()
        for j in range(1, turns):
            weight_x[m, k, j].wait_recv()

    send_weights(0, groups)
    send_weights(1, HELD)
    for m in range(3):
        keep_weights(m)

    normed = root_norm(query_latent[...].astype(F32), query_gain[...]).astype(BF)
    heads = []
    for weight, plain, value_dim, head_count, first_key, first_value in (
        (query_wide, NOPE_B, V_B, heads_w, 0, 0),
        (query_narrow, NOPE_A, V_A, heads_n, heads_w * NOPE_B, wide_v),
    ):
        for h in range(head_count):
            first = h * (plain + ROPE)
            turn_w = weight[first + plain : first + plain + ROPE, :]
            plain_q = across_dot(normed, weight[first : first + plain, :]).astype(BF)
            turn_q = across_dot(normed, turn_w)
            flip_q = across_dot(normed, dot(swap[...], turn_w).astype(BF))
            turn_q = (turn_q * cosine[...] + flip_q * sine[...]).astype(BF)
            query = jnp.concatenate([plain_q, turn_q], axis=1)
            heads.append((query, plain, value_dim, first_key + h * plain, first_value + h * value_dim))
    key_all[0 : heads_w * NOPE_B, :] = key_wide[...].T
    key_all[heads_w * NOPE_B :, :] = key_narrow[...]
    value_all[:, 0:wide_v] = value_wide[...]
    value_all[:, wide_v:] = value_narrow[...].T

    shares = {}

    def to_mate(k, j):
        block = latents.at[source_at(k, j), part]
        copy = send(block, block, lcs.at[k, j], lcr.at[k, j], sp, near)
        copy.start()
        tail.append(copy.wait_send)
        shares[k, j] = copy

    def latent_x(k, j):
        block = latents.at[sp, part]
        return send(block, block, lxs.at[k, j], lxr.at[k, j], turn_at(j), tp)

    for k in range(1, groups):
        lat_copies[k - 1].wait_recv()
        tail.append(lat_copies[k - 1].wait_send)
        block = latents.at[source_at(k, 0), part]
        for j in range(1, turns):
            copy = send(block, block, lxs.at[k, j], lxr.at[k, j], turn_at(j), tp)
            copy.start()
            tail.append(copy.wait_send)
        to_mate(k, 0)
    for m in range(3):
        pass_weights(m, 0)

    per = min(KEY_BLOCK // rows, count)
    blocks = count // per
    peaks[...] = jnp.full(peaks.shape, -jnp.inf, F32)
    tops[...] = jnp.full(tops.shape, -jnp.inf, F32)
    totals[...] = jnp.zeros(totals.shape, F32)
    sums[...] = jnp.zeros(sums.shape, F32)

    def score(shard, slot):
        rows_here = latents[shard, 0:rows, :]
        turned_here = latents[shard, rows : rows + ROPE, :]
        keys = across_dot(key_all[...], rows_here).astype(BF)
        vals[pl.ds(slot * rows, rows), :] = dot(rows_here, value_all[...]).astype(BF)
        for n, (query, plain, _, first_key, _) in enumerate(heads):
            joined = jnp.concatenate([keys[first_key : first_key + plain], turned_here], axis=0)
            scores = dot(query, joined)
            board[n, :, slot * rows : (slot + 1) * rows] = scores
            best = peaks[n]
            for c in range(0, rows, 128):
                best = jnp.maximum(best, scores[:, c : c + 128])
            peaks[n] = best

    def gather_softmax():
        for n, (_, plain, value_dim, _, first_value) in enumerate(heads):
            scale = (plain + ROPE) ** (-0.5) * 1.4426950408889634
            before = tops[n]
            largest = jnp.broadcast_to(jnp.max(peaks[n], axis=-1, keepdims=True), before.shape) * scale
            factor = jnp.exp2(before - largest)
            tops[n] = largest
            totals[n] = totals[n] * factor
            at_v = slice(first_value, first_value + value_dim)
            sums[:, at_v] = sums[:, at_v] * factor[:, 0:1]

            def tile(i, inner):
                at = pl.ds(pl.multiple_of(i * ROW_TILE, ROW_TILE), ROW_TILE)
                top = tops[n, at, :]
                total = totals[n, at, :]
                for c in range(0, per * rows, 128):
                    lifted = jnp.exp2(board[n, at, c : c + 128] * scale - top)
                    total = total + lifted
                    raised[at, c : c + 128] = lifted.astype(BF)
                totals[n, at, :] = total
                return inner

            lax.fori_loop(0, rows // ROW_TILE, tile, 0)
            sums[:, at_v] = sums[:, at_v] + dot(raised[...], vals[:, at_v])

    if blocks == 1:
        slot = 0
        score(sp, slot)
        for k in range(1, groups):
            shares[k, 0].wait_recv()
            slot += 1
            score(source_at(k, 0), slot)
        for k in range(groups):
            for j in range(1, turns):
                latent_x(k, j).wait_recv()
                to_mate(k, j)
        pass_weights(0, 1)
        for k in range(groups):
            for j in range(1, turns):
                shares[k, j].wait_recv()
                slot += 1
                score(source_at(k, j), slot)
        gather_softmax()
    else:
        for k in range(1, groups):
            shares[k, 0].wait_recv()
        for k in range(groups):
            for j in range(1, turns):
                latent_x(k, j).wait_recv()
                to_mate(k, j)
        pass_weights(0, 1)
        for k in range(groups):
            for j in range(1, turns):
                shares[k, j].wait_recv()

        def attend(b, carry):
            for s in range(per):
                score(b * per + s, s)
            gather_softmax()
            return carry

        lax.fori_loop(0, blocks, attend, 0)
    for n, (_, _, value_dim, _, first_value) in enumerate(heads):
        total = jnp.sum(totals[n], axis=-1, keepdims=True)
        result = (sums[:, first_value : first_value + value_dim] / total).astype(BF)
        if first_value < wide_v:
            for t in range(parts):
                place = t * wide_v + first_value

                @pl.when(tp == t)
                def _():
                    att_w[:, place : place + value_dim] = result
        else:
            place = first_value - wide_v
            att_n[tp, :, place : place + value_dim] = result

    rest = [
        share(
            att_w.at[:, pl.ds(pl.multiple_of(tp * wide_v, 128), wide_v)],
            lambda t: att_w.at[:, pl.ds(pl.multiple_of(t * wide_v, 128), wide_v)],
            3,
        ),
        share(att_n.at[tp], lambda t: att_n.at[t], 4),
    ]
    done = [step() for step in onward]
    done += [step() for step in rest]
    for step in done:
        step()
    for i in range(3, 6):
        loads[i].wait()
    for copy in gain_copies:
        copy.wait_recv()

    block_w = width // parts
    narrow = jnp.concatenate([att_n[t] for t in range(parts)], axis=1)
    run = jnp.zeros((rows, 128), F32)
    for c in range(parts):
        at = slice(c * block_w, (c + 1) * block_w)
        mixed = dot(att_w[...], out_w[:, at]) + dot(narrow, out_n[:, at])
        mixed = mixed + DEEP_ALPHA * res_all[c].astype(F32)
        board[0, :, at] = mixed
        for b in range(0, block_w, 128):
            run = run + mixed[:, b : b + 128]
    tops[0] = jnp.broadcast_to(jnp.sum(run, axis=-1, keepdims=True) / width, run.shape)

    def moments(i, inner):
        at = pl.ds(pl.multiple_of(i * ROW_TILE, ROW_TILE), ROW_TILE)
        center = tops[0, at, :]
        square = jnp.zeros(center.shape, F32)
        for c in range(0, width, 128):
            moved = board[0, at, c : c + 128] - center
            square = square + moved * moved
        totals[0, at, :] = square
        return inner

    lax.fori_loop(0, rows // ROW_TILE, moments, 0)
    spread = jnp.sum(totals[0], axis=-1, keepdims=True) / width
    totals[0] = jnp.broadcast_to(lax.rsqrt(spread + EPS_LAYER), totals.shape[1:])

    def first_norm(i, inner):
        at = pl.ds(pl.multiple_of(i * ROW_TILE, ROW_TILE), ROW_TILE)
        center, scale = tops[0, at, :], totals[0, at, :]
        for c in range(0, width, 128):
            t, b = c // block_w, c % block_w
            moved = (board[0, at, c : c + 128] - center) * scale
            moved = moved * gains[t, 0:1, b : b + 128] + gains[t, 1:2, b : b + 128]
            x_all[group, at, c : c + 128] = moved.astype(BF)
        return inner

    lax.fori_loop(0, rows // ROW_TILE, first_norm, 0)

    def strip(t):
        return pl.ds(pl.multiple_of(t * quarter, quarter), quarter)

    def ahead(source, step):
        block = x_all.at[source, strip(tp)]
        target = (group + step) * turns + turn
        return send(block, block, ags.at[source, (step + 1) // 2], agr.at[source], target, tp)

    def maybe(condition, act):
        @pl.when(condition)
        def _():
            act()

    for step in (1, -1):
        inside = (group + step >= 0) & (group + step < groups)
        maybe(inside, lambda step=step: ahead(group, step).start())
        tail.append(
            lambda inside=inside, step=step: maybe(inside, lambda: ahead(group, step).wait_send())
        )
    for k in range(HELD + 1, groups):
        weight_z[1, k].start()
    send_weights(2, 0)

    def start_down(first=1, past=groups):
        for k in range(first, past):
            weight_z[2, k].start()

    start_down(1, 2)
    for k in range(2, groups):
        pass_weights(0, k)
    for k in range(1, groups - 1):
        pass_weights(1, k)

    relayed = {}
    edge = (group == 0) | (group == groups - 1)

    def relay(k, only=None):
        source = sources[k]
        block = x_all.at[source, strip(tp)]
        steps = []
        for step in (1, -1):
            from_behind = source < group if step == 1 else source > group
            inside = from_behind & (group + step >= 0) & (group + step < groups)
            steps.append((inside, ahead(source, step)))
        if (k, 0) not in relayed:
            for i, peer in ((0, far), (1, near)):
                copy = send(block, block, ars.at[k, i], arr.at[k, i], sp, peer)
                tail.append(copy.wait_send)
                relayed[k, i] = copy
            for inside, copy in steps:
                tail.append(lambda inside=inside, copy=copy: maybe(inside, copy.wait_send))

        def act():
            steps[0][1].wait_recv()
            for inside, copy in steps:
                maybe(inside, copy.start)
            for i in range(2):
                relayed[k, i].start()

        if only is None:
            act()
        else:
            maybe(only, act)

    def relay_far(k):
        relayed[k, 0].wait_recv()
        block = x_all.at[sources[k], strip(far)]
        copy = send(block, block, ars.at[k, 2], arr.at[k, 2], sp, near)
        copy.start()
        tail.append(copy.wait_send)
        relayed[k, 2] = copy

    def compute(k):
        if k:
            relayed[k, 1].wait_recv()
            relayed[k, 2].wait_recv()
        gate = jnp.zeros((rows, hidden_count), F32)
        lifted = gate
        for i in range(count):
            columns = x_all[sources[k], :, i * depth : (i + 1) * depth]
            gate += across_dot(columns, weights[0, i])
            lifted += across_dot(columns, weights[1, i])
        hidden[k] = (jax.nn.silu(gate) * lifted).astype(BF)

    span = turns * depth

    def column_group(c):
        return sources[c]

    firsts, seconds, thirds = {}, {}, {}

    def down(c, k):
        for j in range(turns):
            source = column_group(c) * turns + j
            product = dot(hidden[k], weights[2, source])
            parts_f[column_group(c), pl.ds(k * rows, rows), j * depth : (j + 1) * depth] = product
        for h in range(2):
            first = pl.multiple_of(k * rows + (2 * h + 1 - low) * quarter, quarter)
            s1[c, k, h] = parts_f[column_group(c), pl.ds(first, quarter), :].astype(BF)
        firsts[c, k] = send(s1.at[c, k], r1.at[c, k], p1s.at[c, k], p1r.at[c, k], sp, near)
        firsts[c, k].start()
        tail.append(firsts[c, k].wait_send)

    def second(c, k):
        firsts[c, k].wait_recv()
        first = pl.multiple_of(k * rows + (2 * (1 - high) + low) * quarter, quarter)
        kept = parts_f[column_group(c), pl.ds(first, quarter), :]
        s2[c, k] = (kept + r1[c, k, 1 - high].astype(F32)).astype(BF)
        seconds[c, k] = send(s2.at[c, k], r2.at[c, k], p2s.at[c, k], p2r.at[c, k], sp, far)
        seconds[c, k].start()
        tail.append(seconds[c, k].wait_send)

    def third(c, k):
        seconds[c, k].wait_recv()
        first = pl.multiple_of(k * rows + tp * quarter, quarter)
        total = parts_f[column_group(c), pl.ds(first, quarter), :]
        total = total + r1[c, k, high].astype(F32) + r2[c, k].astype(F32)
        if k == 0:
            parts_f[column_group(c), pl.ds(first, quarter), :] = total
        else:
            s3[c, k] = total.astype(BF)
            place = r3.at[column_group(c), group]
            copy = send(
                s3.at[c, k], place, p3s.at[c, k], p3r.at[column_group(c), group],
                sources[k] * turns + turn, tp,
            )
            copy.start()
            tail.append(copy.wait_send)

    waiting, moving = [], []

    def push_second(left):
        while len(waiting) > left:
            second(*waiting[0])
            moving.append(waiting.pop(0))

    def push_third(left):
        while len(moving) > left:
            third(*moving.pop(0))

    def unit(c, k):
        down(c, k)
        waiting.append((c, k))
        push_second(2)
        push_third(6)

    last = groups - 1
    for k in range(1, last):
        relay(k)
        if k == 1:
            pass_weights(1, last)
    maybe(edge, lambda: start_down(2, max(last, 2)))
    if last > 1:
        relay_far(1)
    if last > 0:
        relay(last, ~edge)
    maybe(~edge, lambda: start_down(2, max(last, 2)))
    if last == 1:
        pass_weights(1, last)
    if last > 0:
        pass_weights(2, 1)
    for m in range(2):
        for q in range(groups):
            weights_here(m, q)
    compute(0)
    if last > 1:
        compute(1)
    start_down(max(last, 2))
    weights_here(2, 0)
    early = [*range(1, last), 0]
    if last > 1:
        unit(0, 1)
    unit(0, 0)
    if last > 0:
        push_second(0)
        relay(last, edge)
    for k in range(2, last):
        relay_far(k)
        compute(k)
        unit(0, k)
    if last > 0:
        push_second(0)
        weights_here(2, 1)
        for k in early:
            unit(1, k)
        push_second(0)
        relay_far(last)
        for c in range(2, groups):
            pass_weights(2, c)
        push_third(3)
        compute(last)
        for c in range(2):
            unit(c, last)
    for c in range(2, groups):
        push_second(0)
        if c == 2:
            push_third(4)
        weights_here(2, c)
        for k in [last, *early[:-1]]:
            unit(c, k)
    for c in range(2, groups):
        unit(c, 0)
    push_second(0)
    push_third(0)

    def arrival(c, k):
        place = r3.at[column_group(c), sources[k]]
        return send(
            place, place, p3s.at[c, k], p3r.at[column_group(c), sources[k]], sp, near
        )

    for c in range(groups):
        for k in range(1, groups):
            arrival(c, k).wait_recv()
    gain2 = jnp.concatenate([gains[t, 2:3, :] for t in range(parts)], axis=1)
    bias2 = jnp.concatenate([gains[t, 3:4, :] for t in range(parts)], axis=1)
    for i in range(quarter // ROW_TILE):
        base = pl.multiple_of(tp * quarter + i * ROW_TILE, ROW_TILE)
        at = slice(i * ROW_TILE, (i + 1) * ROW_TILE)
        pieces = []
        for g in range(groups):
            total = parts_f[g, pl.ds(base, ROW_TILE), :]
            for k in range(1, groups):
                total = total + r3[g, sources[k], at, :].astype(F32)
            pieces.append(total)
        total = jnp.concatenate(pieces, axis=1)
        total = total + DEEP_ALPHA * x_all[group, pl.ds(base, ROW_TILE), :].astype(F32)
        result = layer_norm(total, gain2, bias2).astype(BF)
        for c in range(parts):
            final[c, at, :] = result[:, c * block_w : (c + 1) * block_w]
    finals = []
    for i, peer in enumerate((far, diag, near)):
        copy = send(final.at[peer], out_ref.at[strip(tp)], fs.at[i], fr.at[i], sp, peer)
        copy.start()
        finals.append(copy)
    local = pltpu.make_async_copy(final.at[tp], out_ref.at[strip(tp)], fl)
    local.start()
    for copy in finals:
        copy.wait_recv()
        copy.wait_send()
    local.wait()
    for wait in tail:
        wait()


def whole_layer(args, constants, groups, turns, parts):
    (
        residual, query_latent, shared_latent, rotary_key, query_gain, latent_gain,
        query_narrow, key_narrow, value_narrow, query_wide, key_wide, value_wide,
        output_narrow, output_wide, first_gain, first_bias,
        gate_weight, up_weight, down_weight, second_gain, second_bias,
    ) = args
    count = groups * turns
    rows, own_width = residual.shape
    width = own_width * parts
    depth, hidden_local = gate_weight.shape
    hidden_count = hidden_local // groups
    heads_n, heads_w = key_narrow.shape[0] // NOPE_A, key_wide.shape[1] // NOPE_B
    heads = heads_n + heads_w
    quarter = rows // parts
    keys = min(KEY_BLOCK, count * rows)
    latent_width = shared_latent.shape[1]
    dma = pltpu.SemaphoreType.DMA
    far_ref = pl.BlockSpec(memory_space=pl.ANY)
    operands = [*args, *constants]
    staged_inputs = [i for i in range(len(operands)) if i not in (0, 12, 13, 16, 17, 18)]
    strip = (quarter, turns * depth)
    return pl.pallas_call(
        functools.partial(layer_kernel, groups, turns, parts, staged_inputs),
        out_shape=jax.ShapeDtypeStruct(residual.shape, BF),
        in_specs=[far_ref] * len(operands),
        out_specs=far_ref,
        scratch_shapes=[
            pltpu.VMEM((2, depth, hidden_local), BF),
            pltpu.VMEM((3, hidden_local, depth), BF),
            pltpu.VMEM((3, count, hidden_count, depth), BF),
            pltpu.VMEM((count, rows + ROPE, latent_width), BF),
            pltpu.VMEM((rows, ROPE), F32),
            pltpu.VMEM((rows, ROPE), F32),
            pltpu.VMEM((heads, rows, max(width, keys)), F32),
            pltpu.VMEM((groups, groups * rows, turns * depth), F32),
            pltpu.VMEM((rows, keys), BF),
            pltpu.VMEM((heads_w * NOPE_B + heads_n * NOPE_A, latent_width), BF),
            pltpu.VMEM((latent_width, heads_w * V_B + heads_n * V_A), BF),
            pltpu.VMEM((keys, heads_w * V_B + heads_n * V_A), BF),
            pltpu.VMEM((heads, rows, 128), F32),
            pltpu.VMEM((heads, rows, 128), F32),
            pltpu.VMEM((heads, rows, 128), F32),
            pltpu.VMEM((rows, heads_w * V_B + heads_n * V_A), F32),
            pltpu.VMEM((parts * heads_n * V_A, width), BF),
            pltpu.VMEM((parts * heads_w * V_B, width), BF),
            pltpu.VMEM((parts,) + residual.shape, BF),
            pltpu.VMEM((8, own_width), F32),
            pltpu.VMEM((parts, 8, own_width), F32),
            pltpu.VMEM((parts, rows, heads_n * V_A), BF),
            pltpu.VMEM((rows, parts * heads_w * V_B), BF),
            pltpu.VMEM((groups, rows, width), BF),
            pltpu.VMEM((groups, rows, hidden_count), BF),
            pltpu.VMEM((groups, groups, 2) + strip, BF),
            pltpu.VMEM((groups, groups, 2) + strip, BF),
            pltpu.VMEM((groups, groups) + strip, BF),
            pltpu.VMEM((groups, groups) + strip, BF),
            pltpu.VMEM((groups, groups) + strip, BF),
            pltpu.VMEM((groups, groups) + strip, BF),
            pltpu.VMEM((parts, quarter, own_width), BF),
            dma((6,)),
            dma((groups,)),
            dma((groups,)),
            dma((groups, turns)),
            dma((groups, turns)),
            dma((groups, turns)),
            dma((groups, turns)),
            dma((3, groups)),
            dma((3, groups)),
            dma((3, groups, turns)),
            dma((3, groups, turns)),
            dma((3,)),
            dma((5, 3)),
            dma((5, 3)),
            dma((3,)),
            dma((3,)),
            dma((groups, 2)),
            dma((groups,)),
            dma((groups, 3)),
            dma((groups, 3)),
            dma((groups, groups)),
            dma((groups, groups)),
            dma((groups, groups)),
            dma((groups, groups)),
            dma((groups, groups)),
            dma((groups, groups)),
            dma((3,)),
            dma((3,)),
            dma(()),
            *[pltpu.VMEM(operands[i].shape, operands[i].dtype) for i in staged_inputs],
            dma((len(staged_inputs),)),
        ],
        compiler_params=pltpu.CompilerParams(
            collective_id=0, has_side_effects=True, vmem_limit_bytes=62 * 2**20
        ),
        name="layer",
    )(*operands)


def body(*args):
    args = [a.reshape(1, -1) if a.ndim == 1 else a for a in args]
    for i in (3, 6, 7, 8, 9):
        args[i] = args[i].T
    rows, own_width = args[0].shape
    device_count, parts = lax.axis_size("sp"), lax.axis_size("tp")
    hidden_local = args[16].shape[1]
    groups = split_groups(device_count, hidden_local, own_width * parts, rows)
    turns = device_count // groups
    constants = [jnp.asarray(t) for t in axial_tables(rows * device_count)]
    constants.append(jnp.asarray(swap_matrix(), BF))
    return whole_layer(args, constants, groups, turns, parts)


def solution(mesh):
    return jax.shard_map(
        body,
        mesh=mesh,
        in_specs=(
            P("sp", "tp"),
            P("sp", None),
            P("sp", None),
            P("sp", None),
            P(),
            P(),
            P(None, "tp"),
            P(None, "tp"),
            P(None, "tp"),
            P(None, "tp"),
            P(None, "tp"),
            P(None, "tp"),
            P("tp", None),
            P("tp", None),
            P("tp"),
            P("tp"),
            P("sp", "tp"),
            P("sp", "tp"),
            P("tp", "sp"),
            P("tp"),
            P("tp"),
        ),
        out_specs=P("sp", "tp"),
        check_vma=False,
    )
```

```python
import functools

import jax
import jax.numpy as jnp
import numpy as np
from jax import lax
from jax.experimental import pallas as pl
from jax.experimental.pallas import tpu as pltpu
from jax.sharding import PartitionSpec as P

ROPE = 32
NOPE_A = 64
V_A = 64
NOPE_B = 128
V_B = 128
GRID_W = 64

EPS_ROOT = 1e-06
EPS_LAYER = 1e-05
THETA = 10000.0
DEEP_ALPHA = 2.0**0.25

KEY_BLOCK = 2048
ROW_TILE = 16
HELD = 3
MESH = pl.DeviceIdType.MESH
BF = jnp.bfloat16
F32 = jnp.float32


def axial_tables(row_total):
    quarter = ROPE // 4
    freqs = np.float32(THETA) ** (-(2.0 * np.arange(quarter, dtype=np.float32)) / (2 * quarter))
    freqs = freqs.astype(np.float32)

    def spread(count, first):
        angle = np.arange(count, dtype=np.float32)[:, None] * freqs
        out = []
        for fn in (np.cos, np.sin):
            table = np.zeros((count, ROPE), np.float32)
            wave = fn(angle).astype(np.float32)
            start = 0 if first else ROPE // 2
            table[:, start : start + quarter] = wave
            table[:, start + quarter : start + 2 * quarter] = wave
            out.append(table)
        return out

    return spread(row_total // GRID_W, True) + spread(GRID_W, False)


def swap_matrix():
    quarter = ROPE // 4
    swap = np.zeros((ROPE, ROPE), np.float32)
    for base in (0, ROPE // 2):
        for i in range(quarter):
            swap[base + i, base + quarter + i] = -1.0
            swap[base + quarter + i, base + i] = 1.0
    return swap


def split_groups(device_count, hidden_local, width, row_count):
    best = None
    for groups in range(1, device_count + 1):
        if device_count % groups or hidden_local % groups:
            continue
        moved = 3 * width * hidden_local // groups + 2 * row_count * groups * width
        if best is None or moved < best[0]:
            best = (moved, groups)
    return best[1]


def other(index, bit):
    return index + bit * (1 - 2 * ((index // bit) % 2))


def send(source, target, send_sem, recv_sem, sp, tp):
    return pltpu.make_async_remote_copy(
        src_ref=source,
        dst_ref=target,
        send_sem=send_sem,
        recv_sem=recv_sem,
        device_id={"sp": sp, "tp": tp},
        device_id_type=MESH,
    )


def dot(a, b):
    return jnp.dot(a, b, preferred_element_type=F32)


def across_dot(rows, columns):
    return lax.dot_general(
        rows, columns, (((1,), (1,)), ((), ())), preferred_element_type=F32
    )


def root_norm(values, gain):
    return values * lax.rsqrt(jnp.mean(values * values, axis=-1, keepdims=True) + EPS_ROOT) * gain


def layer_norm(values, gain, bias):
    center = jnp.mean(values, axis=-1, keepdims=True)
    moved = values - center
    spread = jnp.mean(moved * moved, axis=-1, keepdims=True)
    return moved * lax.rsqrt(spread + EPS_LAYER) * gain + bias


def chain_orders(groups):
    found = []
    for g in range(groups):
        outward = 1 if 2 * g >= groups else -1
        found.append(sorted(range(groups), key=lambda s: (abs(s - g), (g - s) * outward)))
    return found


def pick(index, options):
    value = options[-1]
    for i, option in enumerate(options[:-1]):
        value = jnp.where(index == i, option, value)
    return value


OPEN_SCOPES = []


def mark(name):
    if OPEN_SCOPES:
        OPEN_SCOPES.pop().__exit__(None, None, None)
    if name:
        scope = jax.named_scope(name)
        scope.__enter__()
        OPEN_SCOPES.append(scope)


def layer_kernel(groups, turns, parts, staged_inputs, *refs):
    inputs, held, fetch_sem = refs[:26], refs[-1 - len(staged_inputs) : -1], refs[-1]
    fetches = []
    for i, place in enumerate(staged_inputs):
        fetch = pltpu.make_async_copy(inputs[place], held[i], fetch_sem.at[i])
        fetch.start()
        fetches.append(fetch)
        inputs = inputs[:place] + (held[i],) + inputs[place + 1 :]
    refs = refs[: -1 - len(staged_inputs)]
    (
        residual, query_latent, shared_latent, rotary_key, query_gain, latent_gain,
        query_narrow, key_narrow, value_narrow, query_wide, key_wide, value_wide,
        output_narrow, output_wide, first_gain, first_bias,
        gate_weight, up_weight, down_weight, second_gain, second_bias,
        row_cos, row_sin, col_cos, col_sin, swap,
    ) = inputs
    out_ref = refs[26]
    (
        raw, staged, weights, latents, cosine, sine, board, parts_f, raised, key_all, value_all, vals,
        peaks, tops, totals, sums, out_n, out_w, res_all, own_gains, gains,
        att_n, att_w, x_all, hidden, s1, r1, s2, r2, s3, r3, final,
    ) = refs[27:59]
    (
        load_sem, lzs, lzr, lxs, lxr, lcs, lcr, wzs, wzr, wxs, wxr, wls,
        tps, tpr, gns, gnr, ags, agr, ars, arr, p1s, p1r, p2s, p2r, p3s, p3r, fs, fr, fl,
    ) = refs[59:]
    sp, tp = lax.axis_index("sp"), lax.axis_index("tp")
    count = groups * turns
    group, turn = sp // turns, sp % turns
    low, high = tp % 2, tp // 2
    near, far = other(tp, 1), other(tp, 2)
    diag = other(far, 1)
    rows = query_latent.shape[0]
    width = residual.shape[1] * parts
    hidden_count, depth = weights.shape[2], weights.shape[3]
    quarter = rows // parts
    orders = chain_orders(groups)
    sources = [group] + [pick(group, [orders[g][k] for g in range(groups)]) for k in range(1, groups)]
    heads_w, heads_n = key_wide.shape[1] // NOPE_B, key_narrow.shape[0] // NOPE_A
    tail = []

    def group_at(k):
        return ((group + k) % groups) * turns + turn

    def turn_at(j):
        return group * turns + (turn + j) % turns

    def source_at(k, j):
        return ((group - k + groups) % groups) * turns + (turn - j + turns) % turns

    mark("a_start")
    wide_v, narrow_v = heads_w * V_B, heads_n * V_A
    own_w = pl.ds(pl.multiple_of(tp * wide_v, 16), wide_v)
    own_n = pl.ds(pl.multiple_of(tp * narrow_v, 16), narrow_v)
    loads = []
    for i, (source, target) in enumerate(
        (
            (gate_weight, raw.at[0]),
            (up_weight, raw.at[1]),
            (down_weight, staged.at[2]),
            (output_narrow, out_n.at[own_n]),
            (output_wide, out_w.at[own_w]),
            (residual, res_all.at[tp]),
        )
    ):
        load = pltpu.make_async_copy(source, target, load_sem.at[i])
        load.start()
        loads.append(load)

    barrier = pltpu.get_barrier_semaphore()
    peers = [(group_at(k), tp) for k in range(1, groups)]
    peers += [(turn_at(j), tp) for j in range(1, turns)]
    peers += [(sp, near), (sp, far), (sp, diag)]
    for a, b in peers:
        pl.semaphore_signal(barrier, inc=1, device_id={"sp": a, "tp": b}, device_id_type=MESH)

    for fetch in fetches:
        fetch.wait()

    grid_rows = rows // GRID_W
    for i in range(grid_rows):
        at = pl.ds(i * GRID_W, GRID_W)
        line = pl.ds(sp * grid_rows + i, 1)
        cosine[at, :] = col_cos[...] + row_cos[line, :]
        sine[at, :] = col_sin[...] + row_sin[line, :]
    latents[sp, 0:rows, :] = root_norm(shared_latent[...].astype(F32), latent_gain[...]).astype(BF)
    rotary = rotary_key[...]
    turned = rotary.astype(F32) * cosine[...].T + dot(swap[...], rotary) * sine[...].T
    latents[sp, rows : rows + ROPE, :] = turned.astype(BF)
    own_gains[...] = jnp.zeros(own_gains.shape, F32)
    for i, ref in enumerate((first_gain, first_bias, second_gain, second_bias)):
        own_gains[i : i + 1, :] = ref[...]
        gains[tp, i : i + 1, :] = ref[...]
    mark("b_barrier")
    pl.semaphore_wait(barrier, len(peers))

    mark("c_send")
    half = (rows + ROPE) // 2
    part = pl.ds(pl.multiple_of(low * half, half), half)
    lat_copies = []
    for k in range(1, groups):
        block = latents.at[sp, part]
        copy = send(block, block, lzs.at[k], lzr.at[k], group_at(k), tp)
        copy.start()
        lat_copies.append(copy)
    for j in range(1, turns):
        block = latents.at[sp, part]
        copy = send(block, block, lxs.at[0, j], lxr.at[0, j], turn_at(j), tp)
        copy.start()
        tail.append(copy.wait_send)

    def share(source, view, i):
        a = send(source, view(tp), tps.at[i, 0], tpr.at[i, 0], sp, far)
        b = send(source, view(tp), tps.at[i, 1], tpr.at[i, 1], sp, near)
        a.start()
        b.start()
        tail.append(a.wait_send)
        tail.append(b.wait_send)

        def onward():
            a.wait_recv()
            c = send(view(far), view(far), tps.at[i, 2], tpr.at[i, 2], sp, near)
            c.start()
            tail.append(c.wait_send)

            def done():
                b.wait_recv()
                c.wait_recv()

            return done

        return onward

    onward = [
        share(output_wide, lambda t: out_w.at[pl.ds(pl.multiple_of(t * wide_v, 16), wide_v)], 0),
        share(output_narrow, lambda t: out_n.at[pl.ds(pl.multiple_of(t * narrow_v, 16), narrow_v)], 1),
        share(residual, lambda t: res_all.at[t], 2),
    ]
    gain_copies = []
    for i, peer in enumerate((near, far, diag)):
        copy = send(own_gains, gains.at[tp], gns.at[i], gnr.at[i], sp, peer)
        copy.start()
        gain_copies.append(copy)
        tail.append(copy.wait_send)

    mark("d_transpose")
    loads[0].wait()
    staged[0] = raw[0].T
    loads[1].wait()
    staged[1] = raw[1].T
    loads[2].wait()

    def piece(m, k):
        first = pl.multiple_of(sources[k] * hidden_count, 16)
        return staged.at[m, pl.ds(first, hidden_count)]

    weight_z = {}

    def keep_weights(m):
        local = pltpu.make_async_copy(piece(m, 0), weights.at[m, sp], wls.at[m])
        local.start()
        weight_z[m, 0] = local

    def send_weights(m, started):
        for k in range(1, groups):
            target = sources[k] * turns + turn
            copy = send(piece(m, k), weights.at[m, sp], wzs.at[m, k], wzr.at[m, group], target, tp)
            if k <= started:
                copy.start()
            tail.append(copy.wait_send)
            weight_z[m, k] = copy

    weight_x = {}

    def pass_weights(m, k):
        source = sources[k] * turns + turn
        block = weights.at[m, source] if k else piece(m, 0)
        if k:
            send(block, block, wzs.at[m, k], wzr.at[m, sources[k]], sp, near).wait_recv()
        for j in range(1, turns):
            copy = send(block, weights.at[m, source], wxs.at[m, k, j], wxr.at[m, k, j], turn_at(j), tp)
            copy.start()
            tail.append(copy.wait_send)
            weight_x[m, k, j] = copy

    def weights_here(m, k):
        if k == 0:
            weight_z[m, 0].wait()
        for j in range(1, turns):
            weight_x[m, k, j].wait_recv()

    send_weights(0, groups)
    send_weights(1, HELD)
    for m in range(3):
        keep_weights(m)

    mark("f_query")
    normed = root_norm(query_latent[...].astype(F32), query_gain[...]).astype(BF)
    heads = []
    for weight, plain, value_dim, head_count, first_key, first_value in (
        (query_wide, NOPE_B, V_B, heads_w, 0, 0),
        (query_narrow, NOPE_A, V_A, heads_n, heads_w * NOPE_B, wide_v),
    ):
        for h in range(head_count):
            first = h * (plain + ROPE)
            turn_w = weight[first + plain : first + plain + ROPE, :]
            plain_q = across_dot(normed, weight[first : first + plain, :]).astype(BF)
            turn_q = across_dot(normed, turn_w)
            flip_q = across_dot(normed, dot(swap[...], turn_w).astype(BF))
            turn_q = (turn_q * cosine[...] + flip_q * sine[...]).astype(BF)
            query = jnp.concatenate([plain_q, turn_q], axis=1)
            heads.append((query, plain, value_dim, first_key + h * plain, first_value + h * value_dim))
    key_all[0 : heads_w * NOPE_B, :] = key_wide[...].T
    key_all[heads_w * NOPE_B :, :] = key_narrow[...]
    value_all[:, 0:wide_v] = value_wide[...]
    value_all[:, wide_v:] = value_narrow[...].T

    mark("e_latz")
    shares = {}

    def to_mate(k, j):
        block = latents.at[source_at(k, j), part]
        copy = send(block, block, lcs.at[k, j], lcr.at[k, j], sp, near)
        copy.start()
        tail.append(copy.wait_send)
        shares[k, j] = copy

    def latent_x(k, j):
        block = latents.at[sp, part]
        return send(block, block, lxs.at[k, j], lxr.at[k, j], turn_at(j), tp)

    for k in range(1, groups):
        lat_copies[k - 1].wait_recv()
        tail.append(lat_copies[k - 1].wait_send)
        block = latents.at[source_at(k, 0), part]
        for j in range(1, turns):
            copy = send(block, block, lxs.at[k, j], lxr.at[k, j], turn_at(j), tp)
            copy.start()
            tail.append(copy.wait_send)
        to_mate(k, 0)
    for m in range(3):
        pass_weights(m, 0)

    per = min(KEY_BLOCK // rows, count)
    blocks = count // per
    peaks[...] = jnp.full(peaks.shape, -jnp.inf, F32)
    tops[...] = jnp.full(tops.shape, -jnp.inf, F32)
    totals[...] = jnp.zeros(totals.shape, F32)
    sums[...] = jnp.zeros(sums.shape, F32)

    def score(shard, slot):
        rows_here = latents[shard, 0:rows, :]
        turned_here = latents[shard, rows : rows + ROPE, :]
        keys = across_dot(key_all[...], rows_here).astype(BF)
        vals[pl.ds(slot * rows, rows), :] = dot(rows_here, value_all[...]).astype(BF)
        for n, (query, plain, _, first_key, _) in enumerate(heads):
            joined = jnp.concatenate([keys[first_key : first_key + plain], turned_here], axis=0)
            scores = dot(query, joined)
            board[n, :, slot * rows : (slot + 1) * rows] = scores
            best = peaks[n]
            for c in range(0, rows, 128):
                best = jnp.maximum(best, scores[:, c : c + 128])
            peaks[n] = best

    def gather_softmax():
        for n, (_, plain, value_dim, _, first_value) in enumerate(heads):
            scale = (plain + ROPE) ** (-0.5) * 1.4426950408889634
            before = tops[n]
            largest = jnp.broadcast_to(jnp.max(peaks[n], axis=-1, keepdims=True), before.shape) * scale
            factor = jnp.exp2(before - largest)
            tops[n] = largest
            totals[n] = totals[n] * factor
            at_v = slice(first_value, first_value + value_dim)
            sums[:, at_v] = sums[:, at_v] * factor[:, 0:1]

            def tile(i, inner):
                at = pl.ds(pl.multiple_of(i * ROW_TILE, ROW_TILE), ROW_TILE)
                top = tops[n, at, :]
                total = totals[n, at, :]
                for c in range(0, per * rows, 128):
                    lifted = jnp.exp2(board[n, at, c : c + 128] * scale - top)
                    total = total + lifted
                    raised[at, c : c + 128] = lifted.astype(BF)
                totals[n, at, :] = total
                return inner

            lax.fori_loop(0, rows // ROW_TILE, tile, 0)
            sums[:, at_v] = sums[:, at_v] + dot(raised[...], vals[:, at_v])

    mark("g_latx")
    if blocks == 1:
        slot = 0
        score(sp, slot)
        for k in range(1, groups):
            shares[k, 0].wait_recv()
            slot += 1
            score(source_at(k, 0), slot)
        mark("g2_latx")
        for k in range(groups):
            for j in range(1, turns):
                latent_x(k, j).wait_recv()
                to_mate(k, j)
        pass_weights(0, 1)
        for k in range(groups):
            for j in range(1, turns):
                shares[k, j].wait_recv()
                slot += 1
                score(source_at(k, j), slot)
        mark("h_attend")
        gather_softmax()
    else:
        for k in range(1, groups):
            shares[k, 0].wait_recv()
        for k in range(groups):
            for j in range(1, turns):
                latent_x(k, j).wait_recv()
                to_mate(k, j)
        pass_weights(0, 1)
        for k in range(groups):
            for j in range(1, turns):
                shares[k, j].wait_recv()

        def attend(b, carry):
            for s in range(per):
                score(b * per + s, s)
            gather_softmax()
            return carry

        lax.fori_loop(0, blocks, attend, 0)
    for n, (_, _, value_dim, _, first_value) in enumerate(heads):
        total = jnp.sum(totals[n], axis=-1, keepdims=True)
        result = (sums[:, first_value : first_value + value_dim] / total).astype(BF)
        if first_value < wide_v:
            for t in range(parts):
                place = t * wide_v + first_value

                @pl.when(tp == t)
                def _():
                    att_w[:, place : place + value_dim] = result
        else:
            place = first_value - wide_v
            att_n[tp, :, place : place + value_dim] = result

    mark("i_share")
    rest = [
        share(
            att_w.at[:, pl.ds(pl.multiple_of(tp * wide_v, 128), wide_v)],
            lambda t: att_w.at[:, pl.ds(pl.multiple_of(t * wide_v, 128), wide_v)],
            3,
        ),
        share(att_n.at[tp], lambda t: att_n.at[t], 4),
    ]
    mark("j_onward")
    done = [step() for step in onward]
    mark("l_attshare")
    done += [step() for step in rest]
    for step in done:
        step()
    for i in range(3, 6):
        loads[i].wait()
    for copy in gain_copies:
        copy.wait_recv()

    mark("m_mixed")
    block_w = width // parts
    narrow = jnp.concatenate([att_n[t] for t in range(parts)], axis=1)
    run = jnp.zeros((rows, 128), F32)
    for c in range(parts):
        at = slice(c * block_w, (c + 1) * block_w)
        mixed = dot(att_w[...], out_w[:, at]) + dot(narrow, out_n[:, at])
        mixed = mixed + DEEP_ALPHA * res_all[c].astype(F32)
        board[0, :, at] = mixed
        for b in range(0, block_w, 128):
            run = run + mixed[:, b : b + 128]
    tops[0] = jnp.broadcast_to(jnp.sum(run, axis=-1, keepdims=True) / width, run.shape)

    def moments(i, inner):
        at = pl.ds(pl.multiple_of(i * ROW_TILE, ROW_TILE), ROW_TILE)
        center = tops[0, at, :]
        square = jnp.zeros(center.shape, F32)
        for c in range(0, width, 128):
            moved = board[0, at, c : c + 128] - center
            square = square + moved * moved
        totals[0, at, :] = square
        return inner

    lax.fori_loop(0, rows // ROW_TILE, moments, 0)
    spread = jnp.sum(totals[0], axis=-1, keepdims=True) / width
    totals[0] = jnp.broadcast_to(lax.rsqrt(spread + EPS_LAYER), totals.shape[1:])

    def first_norm(i, inner):
        at = pl.ds(pl.multiple_of(i * ROW_TILE, ROW_TILE), ROW_TILE)
        center, scale = tops[0, at, :], totals[0, at, :]
        for c in range(0, width, 128):
            t, b = c // block_w, c % block_w
            moved = (board[0, at, c : c + 128] - center) * scale
            moved = moved * gains[t, 0:1, b : b + 128] + gains[t, 1:2, b : b + 128]
            x_all[group, at, c : c + 128] = moved.astype(BF)
        return inner

    lax.fori_loop(0, rows // ROW_TILE, first_norm, 0)

    mark("n_sendrows")
    def strip(t):
        return pl.ds(pl.multiple_of(t * quarter, quarter), quarter)

    def ahead(source, step):
        block = x_all.at[source, strip(tp)]
        target = (group + step) * turns + turn
        return send(block, block, ags.at[source, (step + 1) // 2], agr.at[source], target, tp)

    def maybe(condition, act):
        @pl.when(condition)
        def _():
            act()

    for step in (1, -1):
        inside = (group + step >= 0) & (group + step < groups)
        maybe(inside, lambda step=step: ahead(group, step).start())
        tail.append(
            lambda inside=inside, step=step: maybe(inside, lambda: ahead(group, step).wait_send())
        )
    for k in range(HELD + 1, groups):
        weight_z[1, k].start()
    send_weights(2, 0)

    def start_down(first=1, past=groups):
        for k in range(first, past):
            weight_z[2, k].start()

    start_down(1, 2)
    mark("o_passgate")
    for k in range(2, groups):
        pass_weights(0, k)
    mark("o_passup")
    for k in range(1, groups - 1):
        pass_weights(1, k)

    relayed = {}
    edge = (group == 0) | (group == groups - 1)

    def relay(k, only=None):
        source = sources[k]
        block = x_all.at[source, strip(tp)]
        steps = []
        for step in (1, -1):
            from_behind = source < group if step == 1 else source > group
            inside = from_behind & (group + step >= 0) & (group + step < groups)
            steps.append((inside, ahead(source, step)))
        if (k, 0) not in relayed:
            for i, peer in ((0, far), (1, near)):
                copy = send(block, block, ars.at[k, i], arr.at[k, i], sp, peer)
                tail.append(copy.wait_send)
                relayed[k, i] = copy
            for inside, copy in steps:
                tail.append(lambda inside=inside, copy=copy: maybe(inside, copy.wait_send))

        def act():
            steps[0][1].wait_recv()
            for inside, copy in steps:
                maybe(inside, copy.start)
            for i in range(2):
                relayed[k, i].start()

        if only is None:
            act()
        else:
            maybe(only, act)

    def relay_far(k):
        relayed[k, 0].wait_recv()
        block = x_all.at[sources[k], strip(far)]
        copy = send(block, block, ars.at[k, 2], arr.at[k, 2], sp, near)
        copy.start()
        tail.append(copy.wait_send)
        relayed[k, 2] = copy

    def compute(k):
        if k:
            relayed[k, 1].wait_recv()
            relayed[k, 2].wait_recv()
        gate = jnp.zeros((rows, hidden_count), F32)
        lifted = gate
        for i in range(count):
            columns = x_all[sources[k], :, i * depth : (i + 1) * depth]
            gate += across_dot(columns, weights[0, i])
            lifted += across_dot(columns, weights[1, i])
        hidden[k] = (jax.nn.silu(gate) * lifted).astype(BF)

    span = turns * depth

    def column_group(c):
        return sources[c]

    firsts, seconds, thirds = {}, {}, {}

    def down(c, k):
        for j in range(turns):
            source = column_group(c) * turns + j
            product = dot(hidden[k], weights[2, source])
            parts_f[column_group(c), pl.ds(k * rows, rows), j * depth : (j + 1) * depth] = product
        for h in range(2):
            first = pl.multiple_of(k * rows + (2 * h + 1 - low) * quarter, quarter)
            s1[c, k, h] = parts_f[column_group(c), pl.ds(first, quarter), :].astype(BF)
        firsts[c, k] = send(s1.at[c, k], r1.at[c, k], p1s.at[c, k], p1r.at[c, k], sp, near)
        firsts[c, k].start()
        tail.append(firsts[c, k].wait_send)

    def second(c, k):
        firsts[c, k].wait_recv()
        first = pl.multiple_of(k * rows + (2 * (1 - high) + low) * quarter, quarter)
        kept = parts_f[column_group(c), pl.ds(first, quarter), :]
        s2[c, k] = (kept + r1[c, k, 1 - high].astype(F32)).astype(BF)
        seconds[c, k] = send(s2.at[c, k], r2.at[c, k], p2s.at[c, k], p2r.at[c, k], sp, far)
        seconds[c, k].start()
        tail.append(seconds[c, k].wait_send)

    def third(c, k):
        seconds[c, k].wait_recv()
        first = pl.multiple_of(k * rows + tp * quarter, quarter)
        total = parts_f[column_group(c), pl.ds(first, quarter), :]
        total = total + r1[c, k, high].astype(F32) + r2[c, k].astype(F32)
        if k == 0:
            parts_f[column_group(c), pl.ds(first, quarter), :] = total
        else:
            s3[c, k] = total.astype(BF)
            place = r3.at[column_group(c), group]
            copy = send(
                s3.at[c, k], place, p3s.at[c, k], p3r.at[column_group(c), group],
                sources[k] * turns + turn, tp,
            )
            copy.start()
            tail.append(copy.wait_send)

    waiting, moving = [], []

    def push_second(left):
        while len(waiting) > left:
            second(*waiting[0])
            moving.append(waiting.pop(0))

    def push_third(left):
        while len(moving) > left:
            third(*moving.pop(0))

    def unit(c, k):
        down(c, k)
        waiting.append((c, k))
        push_second(2)
        push_third(6)

    last = groups - 1
    for k in range(1, last):
        mark(f"q{k}_relay")
        relay(k)
        if k == 1:
            mark("q1_passup")
            pass_weights(1, last)
    maybe(edge, lambda: start_down(2, max(last, 2)))
    if last > 1:
        relay_far(1)
    mark("q3_relay")
    if last > 0:
        relay(last, ~edge)
    maybe(~edge, lambda: start_down(2, max(last, 2)))
    if last == 1:
        pass_weights(1, last)
    if last > 0:
        mark("r_pass1")
        pass_weights(2, 1)
    mark("r_weights")
    for m in range(2):
        for q in range(groups):
            weights_here(m, q)
    mark("r_compute")
    compute(0)
    if last > 1:
        compute(1)
    start_down(max(last, 2))
    weights_here(2, 0)
    mark("s_units")
    early = [*range(1, last), 0]
    if last > 1:
        unit(0, 1)
    unit(0, 0)
    if last > 0:
        mark("s_relay3")
        push_second(0)
        relay(last, edge)
    for k in range(2, last):
        mark(f"s{k}_relayfar")
        relay_far(k)
        compute(k)
        unit(0, k)
    if last > 0:
        push_second(0)
        mark("s_units1")
        weights_here(2, 1)
        for k in early:
            unit(1, k)
        push_second(0)
        mark("t1_far3")
        relay_far(last)
        for c in range(2, groups):
            mark(f"t1_pass{c}")
            pass_weights(2, c)
        push_third(3)
        mark("t1_compute3")
        compute(last)
        for c in range(2):
            unit(c, last)
    for c in range(2, groups):
        push_second(0)
        if c == 2:
            push_third(4)
        mark(f"t{c}_wait")
        weights_here(2, c)
        mark(f"t{c}_units")
        for k in [last, *early[:-1]]:
            unit(c, k)
    for c in range(2, groups):
        unit(c, 0)
    mark("u_drain")
    push_second(0)
    push_third(0)

    mark("v_waitthird")
    def arrival(c, k):
        place = r3.at[column_group(c), sources[k]]
        return send(
            place, place, p3s.at[c, k], p3r.at[column_group(c), sources[k]], sp, near
        )

    for c in range(groups):
        for k in range(1, groups):
            arrival(c, k).wait_recv()
    mark("w_norm")
    gain2 = jnp.concatenate([gains[t, 2:3, :] for t in range(parts)], axis=1)
    bias2 = jnp.concatenate([gains[t, 3:4, :] for t in range(parts)], axis=1)
    for i in range(quarter // ROW_TILE):
        base = pl.multiple_of(tp * quarter + i * ROW_TILE, ROW_TILE)
        at = slice(i * ROW_TILE, (i + 1) * ROW_TILE)
        pieces = []
        for g in range(groups):
            total = parts_f[g, pl.ds(base, ROW_TILE), :]
            for k in range(1, groups):
                total = total + r3[g, sources[k], at, :].astype(F32)
            pieces.append(total)
        total = jnp.concatenate(pieces, axis=1)
        total = total + DEEP_ALPHA * x_all[group, pl.ds(base, ROW_TILE), :].astype(F32)
        result = layer_norm(total, gain2, bias2).astype(BF)
        for c in range(parts):
            final[c, at, :] = result[:, c * block_w : (c + 1) * block_w]
    mark("x_finals")
    finals = []
    for i, peer in enumerate((far, diag, near)):
        copy = send(final.at[peer], out_ref.at[strip(tp)], fs.at[i], fr.at[i], sp, peer)
        copy.start()
        finals.append(copy)
    local = pltpu.make_async_copy(final.at[tp], out_ref.at[strip(tp)], fl)
    local.start()
    for copy in finals:
        copy.wait_recv()
        copy.wait_send()
    local.wait()
    mark("y_tail")
    for wait in tail:
        wait()
    mark(None)


def whole_layer(args, constants, groups, turns, parts):
    (
        residual, query_latent, shared_latent, rotary_key, query_gain, latent_gain,
        query_narrow, key_narrow, value_narrow, query_wide, key_wide, value_wide,
        output_narrow, output_wide, first_gain, first_bias,
        gate_weight, up_weight, down_weight, second_gain, second_bias,
    ) = args
    count = groups * turns
    rows, own_width = residual.shape
    width = own_width * parts
    depth, hidden_local = gate_weight.shape
    hidden_count = hidden_local // groups
    heads_n, heads_w = key_narrow.shape[0] // NOPE_A, key_wide.shape[1] // NOPE_B
    heads = heads_n + heads_w
    quarter = rows // parts
    keys = min(KEY_BLOCK, count * rows)
    latent_width = shared_latent.shape[1]
    dma = pltpu.SemaphoreType.DMA
    far_ref = pl.BlockSpec(memory_space=pl.ANY)
    operands = [*args, *constants]
    staged_inputs = [i for i in range(len(operands)) if i not in (0, 12, 13, 16, 17, 18)]
    strip = (quarter, turns * depth)
    return pl.pallas_call(
        functools.partial(layer_kernel, groups, turns, parts, staged_inputs),
        out_shape=jax.ShapeDtypeStruct(residual.shape, BF),
        in_specs=[far_ref] * len(operands),
        out_specs=far_ref,
        scratch_shapes=[
            pltpu.VMEM((2, depth, hidden_local), BF),
            pltpu.VMEM((3, hidden_local, depth), BF),
            pltpu.VMEM((3, count, hidden_count, depth), BF),
            pltpu.VMEM((count, rows + ROPE, latent_width), BF),
            pltpu.VMEM((rows, ROPE), F32),
            pltpu.VMEM((rows, ROPE), F32),
            pltpu.VMEM((heads, rows, max(width, keys)), F32),
            pltpu.VMEM((groups, groups * rows, turns * depth), F32),
            pltpu.VMEM((rows, keys), BF),
            pltpu.VMEM((heads_w * NOPE_B + heads_n * NOPE_A, latent_width), BF),
            pltpu.VMEM((latent_width, heads_w * V_B + heads_n * V_A), BF),
            pltpu.VMEM((keys, heads_w * V_B + heads_n * V_A), BF),
            pltpu.VMEM((heads, rows, 128), F32),
            pltpu.VMEM((heads, rows, 128), F32),
            pltpu.VMEM((heads, rows, 128), F32),
            pltpu.VMEM((rows, heads_w * V_B + heads_n * V_A), F32),
            pltpu.VMEM((parts * heads_n * V_A, width), BF),
            pltpu.VMEM((parts * heads_w * V_B, width), BF),
            pltpu.VMEM((parts,) + residual.shape, BF),
            pltpu.VMEM((8, own_width), F32),
            pltpu.VMEM((parts, 8, own_width), F32),
            pltpu.VMEM((parts, rows, heads_n * V_A), BF),
            pltpu.VMEM((rows, parts * heads_w * V_B), BF),
            pltpu.VMEM((groups, rows, width), BF),
            pltpu.VMEM((groups, rows, hidden_count), BF),
            pltpu.VMEM((groups, groups, 2) + strip, BF),
            pltpu.VMEM((groups, groups, 2) + strip, BF),
            pltpu.VMEM((groups, groups) + strip, BF),
            pltpu.VMEM((groups, groups) + strip, BF),
            pltpu.VMEM((groups, groups) + strip, BF),
            pltpu.VMEM((groups, groups) + strip, BF),
            pltpu.VMEM((parts, quarter, own_width), BF),
            dma((6,)),
            dma((groups,)),
            dma((groups,)),
            dma((groups, turns)),
            dma((groups, turns)),
            dma((groups, turns)),
            dma((groups, turns)),
            dma((3, groups)),
            dma((3, groups)),
            dma((3, groups, turns)),
            dma((3, groups, turns)),
            dma((3,)),
            dma((5, 3)),
            dma((5, 3)),
            dma((3,)),
            dma((3,)),
            dma((groups, 2)),
            dma((groups,)),
            dma((groups, 3)),
            dma((groups, 3)),
            dma((groups, groups)),
            dma((groups, groups)),
            dma((groups, groups)),
            dma((groups, groups)),
            dma((groups, groups)),
            dma((groups, groups)),
            dma((3,)),
            dma((3,)),
            dma(()),
            *[pltpu.VMEM(operands[i].shape, operands[i].dtype) for i in staged_inputs],
            dma((len(staged_inputs),)),
        ],
        compiler_params=pltpu.CompilerParams(
            collective_id=0, has_side_effects=True, vmem_limit_bytes=62 * 2**20
        ),
        name="layer",
    )(*operands)


def body(*args):
    args = [a.reshape(1, -1) if a.ndim == 1 else a for a in args]
    for i in (3, 6, 7, 8, 9):
        args[i] = args[i].T
    rows, own_width = args[0].shape
    device_count, parts = lax.axis_size("sp"), lax.axis_size("tp")
    hidden_local = args[16].shape[1]
    groups = split_groups(device_count, hidden_local, own_width * parts, rows)
    turns = device_count // groups
    constants = [jnp.asarray(t) for t in axial_tables(rows * device_count)]
    constants.append(jnp.asarray(swap_matrix(), BF))
    return whole_layer(args, constants, groups, turns, parts)


def solution(mesh):
    return jax.shard_map(
        body,
        mesh=mesh,
        in_specs=(
            P("sp", "tp"),
            P("sp", None),
            P("sp", None),
            P("sp", None),
            P(),
            P(),
            P(None, "tp"),
            P(None, "tp"),
            P(None, "tp"),
            P(None, "tp"),
            P(None, "tp"),
            P(None, "tp"),
            P("tp", None),
            P("tp", None),
            P("tp"),
            P("tp"),
            P("sp", "tp"),
            P("sp", "tp"),
            P("tp", "sp"),
            P("tp"),
            P("tp"),
        ),
        out_specs=P("sp", "tp"),
        check_vma=False,
    )
```
